512 devices in a mesh: ep: 32 (over z, x), tp: 16 (over y, core).
Axes of the slice: x: 4, y: 8, z: 8, core: 2. Of those that a mesh axis runs over, the one named last changes fastest.
Arguments:
- mix_query: bfloat16 [8192, 2048], P('ep', 'tp'), may hold values from -6 to 6
- forget_input: bfloat16 [8192, 2048], P('ep', 'tp'), may hold values from -6 to 6
- mix_value: bfloat16 [8192, 2048], P('ep', 'tp'), may hold values from -6 to 6
- out_gate_input: bfloat16 [8192, 2048], P('ep', 'tp'), may hold values from -6 to 6
- decay_shift: float32 [8192, 16], P('ep', 'tp'), may hold values from -1.5 to 0
- forget_floor: float32 [2048], P('tp'), may hold values from 0.9 to 1
- head_gain: float32 [128], replicated, may hold values from 0.1 to 1.9
- w_mix_out: bfloat16 [2048, 2048], P(None, 'tp'), may hold values from -0.125 to 0.125
- moe_input: bfloat16 [8192, 2048], P('ep'), may hold values from -6 to 6
- moe_gain: float32 [2048], replicated, may hold values from 0.1 to 1.9
- routes: int32 [8192, 2], P('ep'), may hold values from 0 to 31, all different within a row; in each aligned block of 256 rows (0 to 255, 256 to 511, ...) at most 20 rows name the same one
- route_weight: float32 [8192, 2], P('ep'), may hold values from 0.1 to 1
- w_exp_gate: bfloat16 [32, 2048, 4096], P('ep', None, 'tp'), may hold values from -0.125 to 0.125
- w_exp_up: bfloat16 [32, 2048, 4096], P('ep', None, 'tp'), may hold values from -0.125 to 0.125
- w_exp_down: bfloat16 [32, 4096, 2048], P('ep', 'tp'), may hold values from -0.125 to 0.125
Outputs:
- mixed: bfloat16 [8192, 2048], P('ep', 'tp')
- moe_out: bfloat16 [8192, 2048], P('ep', 'tp')
The draws below stay inside these ranges and needn't reach their ends.
Inputs may be any that keep to these rules, and one draw needn't show every extreme that they name: `routes`: at most 20 of the rows of one index of ep name one expert, and in every draw some device's rows name one expert exactly 20 times; the experts of a row differ.
All inputs are finite; a program needn't handle non-finite values.
Results may differ from the reference program's by a relative error of at most 0.02.
Values may be sent and summed in bfloat16 or wider, within the bound.
A program may use at most 64 MiB of HBM per device.

```python
import math
import jax
import jax.numpy as jnp
import numpy as np
from jax import lax

D = 2048
HEADS = 16
DK = 128
FE = 4096
TOP_K = 2
BLOCK = 64
TOK_DEV = 256
HW = 2048
TOKENS = 8192
EXPERTS = 32
CAP = 20
N_EP = 32
N_TP = 16


def draw_forget_floor(key, part):
    length = TOK_DEV * N_EP
    subkeys = jax.random.split(key, 3)
    fast_share = 0.5
    fast_heads = jax.random.bernoulli(subkeys[0], fast_share, (HEADS,))
    fast_rate = jnp.exp(jax.random.uniform(subkeys[1], (HEADS, DK), jnp.float32, math.log(0.02), math.log(0.07)))
    slow_rate = jnp.exp(jax.random.uniform(subkeys[2], (HEADS, DK), jnp.float32, math.log(0.3), 0.0)) / length
    keep_rate = jnp.where(fast_heads[:, None], fast_rate, slow_rate)
    return (1.0 - keep_rate).reshape(HEADS * DK).astype(jnp.float32)


def draw_decay_shift(key, part):
    length = TOK_DEV * N_EP
    subkeys = jax.random.split(key, 3)
    factor = jnp.exp(jax.random.uniform(subkeys[0], (N_EP, HEADS), jnp.float32, -math.log(2.0), math.log(2.0)))
    steady = -0.4 * jnp.repeat(factor, TOK_DEV, axis=0) / length
    places = jax.random.randint(subkeys[1], (2, HEADS), 0, length)
    depths = jnp.log(jax.random.uniform(subkeys[2], (2, HEADS), jnp.float32, 0.55, 0.8))
    marked = (jnp.arange(length)[:, None, None] == places[None, :, :]).astype(jnp.float32)
    return (steady + jnp.sum(marked * depths[None, :, :], axis=1)).astype(jnp.float32)


def spiked(result, stream_key, source, target, blocks, factor):
    owner, partner = [(jnp.arange(result.shape[axis_at]) // (result.shape[axis_at] // blocks)).reshape([-1 if axis == axis_at else 1 for axis in range(result.ndim)]) for axis_at in (source, target)]
    chosen = jax.random.permutation(stream_key, blocks)[partner]
    strong = (owner == chosen) | (owner == (partner + blocks // 2) % blocks)
    return jnp.where(strong, factor * result, result)


def block_levels(own_key, extent, pieces, smallest, largest):
    loudness = 1.0
    for dim, shards_of in pieces:
        draws = jax.random.uniform(jax.random.fold_in(jax.random.fold_in(own_key, 6), dim), (shards_of,), jnp.float32, smallest / len(pieces), largest / len(pieces))
        loudness = loudness * jnp.repeat(jnp.exp(draws), extent[dim] // shards_of).reshape((-1,) + (1,) * (len(extent) - 1 - dim))
    return loudness


def assign_block(stream_key, own, number, rows, amount, top, reach, slope):
    sequence = jax.random.permutation(stream_key, amount)
    heavy_load, common = shares(amount, rows * top, reach, slope, True), shares(amount, rows * top, reach, slope, False)
    places = jnp.arange(amount)

    def named(tallies, offset_by):
        used = int((tallies > 0).sum())
        fixed = max(1, used // 4)
        moved = fixed + (places - fixed + offset_by * (used - fixed)) % max(1, amount - fixed)
        return jnp.zeros((amount,), jnp.int32).at[sequence[jnp.where(places < fixed, places, moved)]].set(jnp.asarray(tallies, jnp.int32))

    tallies = jnp.where(number % 4 == 0, named(heavy_load, number // 4), named(common, number - number // 4 - 1))
    mixed = jax.random.permutation(jax.random.fold_in(own, 3), amount)
    donor, taker = mixed[0:amount // 2 * 2:2], mixed[1:amount // 2 * 2:2]
    margin = jnp.minimum(tallies[donor] - 1, reach - tallies[taker]) // 2
    margin = jnp.where((donor == sequence[0]) | (taker == sequence[0]) | (tallies[taker] == 0), 0, jnp.maximum(margin, 0))
    moved = jax.random.randint(jax.random.fold_in(own, 4), (amount // 2,), 0, 1 << 20) % (margin + 1)
    tallies = tallies.at[donor].add(-moved).at[taker].add(moved)
    labels = jnp.searchsorted(jnp.cumsum(tallies), jnp.arange(rows * top), side="right").astype(jnp.int32)
    grid = labels.reshape(top, rows).T
    grid = grid[jax.random.permutation(jax.random.fold_in(own, 1), rows)]
    offset_by = jax.random.randint(jax.random.fold_in(own, 2), (rows, 1), 0, top)
    return jnp.take_along_axis(grid, (jnp.arange(top)[None, :] + offset_by) % top, axis=1)


def shares(number_of, total, bound, skew, full):
    portions = [(1 << 20) // math.isqrt(rank ** skew) + 1 for rank in range(1, number_of + 1)]
    largest = bound if full else min(bound, max(-(-total // number_of), total * portions[0] // sum(portions)))
    least = 1 if total - largest >= number_of - 1 else 0
    given, rest = [largest] + [least] * (number_of - 1), total - largest - least * (number_of - 1)
    while rest > 0:
        movable = [i for i in range(1, number_of) if given[i] < largest] or [i for i in range(1, number_of) if given[i] < bound]
        mass, remaining = sum([portions[i] for i in movable]), rest
        for i in movable:
            addition = min(bound - given[i], max(1, remaining * portions[i] // mass), rest)
            given[i] = given[i] + addition
            rest = rest - addition
    return np.array(given)


def centred(stream_key, extent, scale, bound, pieces=(), kind=jnp.bfloat16):
    drawn = scale * jax.random.normal(stream_key, extent, jnp.float32)
    if pieces:
        drawn = drawn * block_levels(stream_key, extent, pieces, -0.22, 0.18)
    return jnp.clip(drawn, -bound, bound).astype(kind)


def bell_draw_with(key, shape, scale, reach, cuts, heavy, held_as=jnp.bfloat16):
    values = scale * jax.random.normal(key, shape, jnp.float32)
    if cuts:
        values = values * block_levels(key, shape, cuts, -0.22, 0.18)
    return jnp.clip(spiked(values, jax.random.fold_in(key, 3), *heavy), -reach, reach).astype(held_as)


def setup_inputs(seed: int = 0) -> dict:
    key_of = jax.random.split(jax.random.key(seed), 16)
    mix_query = centred(key_of[0], (TOKENS, HW), 1.0, 6.0, ((0, 32), (1, 16)))
    forget_input = centred(key_of[1], (TOKENS, HW), 1.0, 6.0, ((0, 32), (1, 16)))
    mix_value = centred(key_of[2], (TOKENS, HW), 1.0, 6.0, ((0, 32), (1, 16)))
    out_gate_input = centred(key_of[3], (TOKENS, HW), 1.0, 6.0, ((0, 32), (1, 16)))
    decay_shift = draw_decay_shift(jax.random.fold_in(key_of[15], 71), 0)
    forget_floor = draw_forget_floor(jax.random.fold_in(key_of[15], 71), 0)
    head_gain = jnp.clip(1.0 + 0.18 * jax.random.normal(key_of[6], (DK,), jnp.float32), 0.1, 1.9)
    w_mix_out = centred(key_of[7], (HW, D), HW ** -0.5, 0.125, ((1, 16),))
    moe_input = centred(key_of[8], (TOKENS, D), 1.0, 6.0, ((0, 32),))
    moe_gain = jnp.clip(1.0 + 0.18 * jax.random.normal(key_of[9], (D,), jnp.float32), 0.1, 1.9)
    routes_keys = jax.random.split(jax.random.fold_in(key_of[10], 1), TOKENS // TOK_DEV)
    routes_turns = jax.random.permutation(jax.random.fold_in(key_of[10], 3), TOKENS // TOK_DEV)
    routes = jax.vmap(lambda own, number: assign_block(jax.random.fold_in(key_of[10], 2), own, number, TOK_DEV, EXPERTS, TOP_K, CAP, 1))(routes_keys, routes_turns).reshape((TOKENS, TOP_K))
    route_weight = jnp.clip(0.1 + 0.9 * jax.random.uniform(key_of[11], (TOKENS, TOP_K), jnp.float32) ** block_levels(key_of[11], (TOKENS, TOP_K), ((0, 32),), -0.2, 0.2), 0.1, 1.0)
    w_exp_gate = centred(key_of[12], (EXPERTS, D, FE), D ** -0.5, 0.125, ((0, 32), (2, 16)))
    w_exp_up = centred(key_of[13], (EXPERTS, D, FE), D ** -0.5, 0.125, ((0, 32), (2, 16)))
    w_exp_down = bell_draw_with(key_of[14], (EXPERTS, FE, D), FE ** -0.5, 0.125, ((0, 32), (1, 16)), (1, 2, 16, 2.0))
    return {"mix_query": mix_query, "forget_input": forget_input, "mix_value": mix_value, "out_gate_input": out_gate_input, "decay_shift": decay_shift, "forget_floor": forget_floor, "head_gain": head_gain, "w_mix_out": w_mix_out, "moe_input": moe_input, "moe_gain": moe_gain, "routes": routes, "route_weight": route_weight, "w_exp_gate": w_exp_gate, "w_exp_up": w_exp_up, "w_exp_down": w_exp_down}


eps = 1e-06
highest_precision = lax.Precision.HIGHEST

def recurrence(query, input_gate, values, log_decay):
    length = query.shape[0]
    blocks = length // BLOCK

    def to_blocks(array):
        return array.reshape(blocks, BLOCK, HEADS, DK).transpose(0, 2, 1, 3)
    causal = jnp.tril(jnp.ones((BLOCK, BLOCK), bool))[:, :, None]

    def advance(recurrent_state, inputs):
        query_block, key_block, value_block, g_block = inputs
        running_decay = jnp.cumsum(g_block, axis=1)
        spread = running_decay[:, :, None, :] - running_decay[:, None, :, :]
        weights = jnp.where(causal, jnp.exp(jnp.minimum(spread, 0.0)), 0.0)
        scores = jnp.einsum('htk,htsk,hsk->hts', query_block, weights, key_block, precision=highest_precision)
        block_result = jnp.einsum('hts,hsv->htv', scores, value_block, precision=highest_precision)
        block_result = block_result + jnp.einsum('rsd,rda->rsa', query_block * jnp.exp(running_decay), recurrent_state, precision=highest_precision)
        closing_total = running_decay[:, -1:, :]
        carried_over_state = jnp.einsum('gbx,gbi->gxi', key_block * jnp.exp(closing_total - running_decay), value_block, precision=highest_precision)
        recurrent_state = jnp.exp(closing_total[:, 0, :])[:, :, None] * recurrent_state + carried_over_state
        return (recurrent_state, block_result)
    initial = jnp.zeros((HEADS, DK, DK), jnp.float32)
    _, block_result = lax.scan(advance, initial, (to_blocks(query), to_blocks(input_gate), to_blocks(values), to_blocks(log_decay)))
    return block_result.transpose(0, 2, 1, 3).reshape(length, HEADS, DK)

def token_mixer(mix_query, forget_input, mix_value, out_gate_input, decay_shift, forget_floor, head_gain, w_mix_out):
    length = mix_query.shape[0]
    gate_input = forget_input.astype(jnp.float32)
    forget = forget_floor + (1.0 - forget_floor) * jax.nn.sigmoid(gate_input)
    input_gate = (1.0 - forget_floor) * jax.nn.sigmoid(-gate_input)
    log_decay = jnp.log(forget) + jnp.repeat(decay_shift, DK, axis=1)
    block_result = recurrence(mix_query.astype(jnp.float32), input_gate, mix_value.astype(jnp.float32), log_decay)
    inverse = lax.rsqrt(lax.optimization_barrier(jnp.mean(block_result * block_result, axis=2, keepdims=True)) + eps)
    gated = jax.nn.silu(out_gate_input.astype(jnp.float32)).reshape(length, HEADS, DK)
    head_out = (block_result * inverse * head_gain * gated).reshape(length, HEADS * DK).astype(jnp.bfloat16)
    return jnp.dot(head_out, w_mix_out, preferred_element_type=jnp.float32).astype(jnp.bfloat16)

def experts_layer(moe_input, moe_gain, routes, route_weight, w_exp_gate, w_exp_up, w_exp_down):
    token_rows = moe_input.astype(jnp.float32)
    inverse = lax.rsqrt(lax.optimization_barrier(jnp.mean(token_rows * token_rows, axis=1, keepdims=True)) + eps)
    normed = (token_rows * inverse * moe_gain).astype(jnp.bfloat16)
    flat_ids = routes.reshape(-1)
    pair_count = flat_ids.shape[0]
    slot_count = CAP * N_EP
    group_size = FE // N_TP

    def one_expert(expert):
        matches = flat_ids == expert
        chosen = jnp.nonzero(matches, size=slot_count, fill_value=0)[0].astype(jnp.int32)
        how_many = jnp.sum(matches.astype(jnp.int32))
        usable = jnp.arange(slot_count, dtype=jnp.int32) < how_many
        picked = normed[chosen // TOP_K]
        gate_sum = jnp.dot(picked, w_exp_gate[expert], preferred_element_type=jnp.float32)
        up_sum = jnp.dot(picked, w_exp_up[expert], preferred_element_type=jnp.float32)
        hidden = (jax.nn.silu(gate_sum) * up_sum).astype(jnp.bfloat16)
        grouped = hidden.reshape(slot_count, N_TP, group_size).astype(jnp.float32)
        down_groups = w_exp_down[expert].reshape(N_TP, group_size, D).astype(jnp.float32)
        partial_value = jnp.einsum('sgf,gfd->sgd', grouped, down_groups).astype(jnp.bfloat16)
        summed = lax.optimization_barrier(jnp.sum(partial_value.astype(jnp.float32), axis=1)).astype(jnp.bfloat16)
        return (chosen, jnp.where(usable[:, None], summed, jnp.zeros_like(summed)))
    chosen_all, outputs = lax.map(one_expert, jnp.arange(EXPERTS, dtype=jnp.int32))
    pair_out = jnp.zeros((pair_count, D), jnp.float32).at[chosen_all.reshape(-1)].add(outputs.reshape(-1, D).astype(jnp.float32))
    combined = lax.optimization_barrier(jnp.sum(pair_out.reshape(-1, TOP_K, D) * route_weight[:, :, None], axis=1))
    return combined.astype(jnp.bfloat16)

def reference(mix_query, forget_input, mix_value, out_gate_input, decay_shift, forget_floor, head_gain, w_mix_out, moe_input, moe_gain, routes, route_weight, w_exp_gate, w_exp_up, w_exp_down):
    mixed = token_mixer(mix_query, forget_input, mix_value, out_gate_input, decay_shift, forget_floor, head_gain, w_mix_out)
    moe_out = experts_layer(moe_input, moe_gain, routes, route_weight, w_exp_gate, w_exp_up, w_exp_down)
    return (mixed, moe_out)
```

```python
import jax
import jax.numpy as jnp
from jax import lax
from jax.experimental import pallas as pl
from jax.experimental.pallas import tpu as pltpu
from jax.sharding import Mesh
from jax.sharding import PartitionSpec as P

EP = ("ep_0", "ep_1")
TP = ("tp_0", "tp_1")
NZ, NX, NY = 8, 4, 8
N_EP = NZ * NX
ROWS = 256
CAP = 20
D = 2048
DK = 128
FPD = 256
HALF = CAP * N_EP // 2
SLOTS = CAP * N_EP
DBLK = 48
RBLK = 32
SUB = 64
PACK = DK + 16
EPS = 1e-6
MESH = pl.DeviceIdType.MESH
F32 = jnp.float32
BF16 = jnp.bfloat16
I32 = jnp.int32
HIGH = lax.Precision.HIGHEST

SEND_ORDER = (8, 7, 9, 6, 10, 5, 11, 4, 12, 3, 13, 2, 14, 1, 15, 0)
RETURN_ORDER = sorted(range(1, N_EP), key=lambda o: -min(o, N_EP - o))
CHUNK_ORDER = (4, 3, 5, 2, 6, 1, 7, 0)


def ones_where(mask):
    return jnp.where(mask, 1.0, 0.0).astype(BF16)


def nt_dot(a, b, precision=None):
    return lax.dot_general(
        a, b, (((1,), (1,)), ((), ())), precision=precision, preferred_element_type=F32
    )


def mm(a, b, precision=None):
    return jnp.dot(a, b, precision=precision, preferred_element_type=F32)


def iota(shape, dim):
    return lax.broadcasted_iota(I32, shape, dim)


def kernel(
    q_ref, f_ref, v_ref, og_ref, shift_ref, floor_ref, hgain_ref, wmix_hbm,
    moe_hbm, gain_ref, routes_ref, rw_ref, wg_hbm, wu_hbm, wd_hbm,
    mixed_ref, moe_ref,
    moe_v, mine_v, wg_v, wu_v, wd_v, wmix_v, norm_v,
    sbuf, rbuf, xs, accg, accu, hid, part, pout, pin, rsend, rrecv,
    rout, rin, qh_v, ql_v, sx, sz, qd_v, hs,
    lsem, wsem, dsend, drecv, asend, arecv, psend, precv, csend, crecv,
    ssend, srecv, bsend, brecv, xsend, xrecv, zsend, zrecv, hsend, hrecv,
    gsend, grecv,
):
    z = lax.axis_index("ep_0")
    x = lax.axis_index("ep_1")
    y = lax.axis_index("tp_0")
    c = lax.axis_index("tp_1")
    me = z * NX + x

    def at_ep(e):
        return (lax.div(e, NX), lax.rem(e, NX), y, c)

    up = (z, x, lax.rem(y + 1, NY), c)
    down = (z, x, lax.rem(y + NY - 1, NY), c)
    partner = (z, x, y, 1 - c)

    def remote(src, dst, send, recv, device):
        return pltpu.make_async_remote_copy(
            src_ref=src, dst_ref=dst, send_sem=send, recv_sem=recv,
            device_id=device, device_id_type=MESH,
        )

    pending = []

    def push(src, dst, send, recv, device):
        copy = remote(src, dst, send, recv, device)
        copy.start()
        pending.append(copy)

    def await_in(dst, send, recv):
        remote(dst, dst, send, recv, partner).wait_recv()

    rows_in = []
    for i in range(4):
        rows_in.append(pltpu.make_async_copy(
            moe_hbm.at[pl.ds(64 * i, 64), :], moe_v.at[pl.ds(64 * i, 64), :], lsem.at[i]))
    rows_in.append(pltpu.make_async_copy(
        moe_hbm.at[:, pl.ds(pl.multiple_of(y * FPD, FPD), FPD)], mine_v, lsem.at[4]))
    for copy in rows_in:
        copy.start()

    barrier = pltpu.get_barrier_semaphore()

    def greet(o, carry):
        pl.semaphore_signal(
            barrier, inc=1, device_id=at_ep(lax.rem(me + o, N_EP)), device_id_type=MESH)
        return carry

    lax.fori_loop(1, N_EP, greet, 0)
    for device in (up, down, partner):
        pl.semaphore_signal(barrier, inc=1, device_id=device, device_id_type=MESH)

    weights_in = [
        pltpu.make_async_copy(wg_hbm, wg_v, wsem.at[0]),
        pltpu.make_async_copy(wu_hbm, wu_v, wsem.at[1]),
        pltpu.make_async_copy(wmix_hbm, wmix_v, wsem.at[2]),
    ]
    for i in range(NY):
        for h in range(2):
            column = pl.multiple_of(i * FPD + lax.rem(c + h, 2) * DK, DK)
            weights_in.append(pltpu.make_async_copy(
                wd_hbm.at[:, pl.ds(column, DK)],
                wd_v.at[i, :, pl.ds(h * DK, DK)], wsem.at[3 + 2 * i + h]))
    for copy in weights_in:
        copy.start()

    e0, e1 = routes_ref[0:1, :], routes_ref[1:2, :]
    ids = iota((N_EP, ROWS), 0)
    one0, one1 = ids == e0, ids == e1
    ones = jnp.concatenate([ones_where(one0), ones_where(one1)], axis=0)
    strict = ones_where(iota((ROWS, ROWS), 0) < iota((ROWS, ROWS), 1))
    earlier = mm(ones, strict)
    total0 = jnp.sum(jnp.where(one0, 1.0, 0.0), axis=1, keepdims=True)
    rank0 = jnp.sum(jnp.where(one0, earlier[:N_EP], 0.0), axis=0, keepdims=True).astype(I32)
    rank1 = jnp.sum(
        jnp.where(one1, earlier[N_EP:] + total0, 0.0), axis=0, keepdims=True).astype(I32)

    for i in range(4):
        rows_in[i].wait()
    rows_in[4].wait()
    gain = gain_ref[pl.ds(y, 1), :]
    for i in range(4):
        block = moe_v[64 * i:64 * i + 64, :].astype(F32)
        mean = jnp.sum(block * block, axis=1, keepdims=True) * (1.0 / D)
        own = mine_v[64 * i:64 * i + 64, :].astype(F32)
        norm_v[64 * i:64 * i + 64, :] = (own * lax.rsqrt(mean + EPS) * gain).astype(BF16)

    parity = lax.rem(x + c, 2)
    target0 = jnp.where((e0 & 1) == parity, (e0 >> 1) * DBLK + rank0, -1000)
    target1 = jnp.where((e1 & 1) == parity, (e1 >> 1) * DBLK + rank1, -1000)
    n0, n1 = norm_v[:, :DK], norm_v[:, DK:]
    for g in range(4):
        spot = iota((4 * DBLK, ROWS), 0) + 4 * DBLK * g
        first = ones_where((spot == target0) | (spot == target1))
        second = ones_where((spot == target0 + CAP) | (spot == target1 + CAP))
        rows = (mm(first, n0) + mm(second, n1)).astype(BF16)
        sbuf[4 * g:4 * g + 4] = rows.reshape(4, DBLK, DK)

    pl.semaphore_wait(barrier, N_EP + 2)

    def dispatch(o):
        expert = lax.rem(me + 2 * o + c, N_EP)
        return remote(sbuf.at[lax.div(expert, 2)], rbuf.at[lax.div(me, 2)],
                      dsend.at[o], drecv.at[o], at_ep(expert))

    own_copy = pltpu.make_async_copy(
        sbuf.at[lax.div(me, 2)], rbuf.at[lax.div(me, 2)], lsem.at[5])
    for o in SEND_ORDER:
        if o:
            dispatch(o).start()
        else:
            @pl.when(c == 1)
            def _():
                dispatch(0).start()

            @pl.when(c == 0)
            def _():
                own_copy.start()

    floor = floor_ref[...]
    pre = f_ref[...].astype(F32)
    forget = floor + (1.0 - floor) * jax.nn.sigmoid(pre)
    keys = (1.0 - floor) * jax.nn.sigmoid(-pre)
    shift = jnp.transpose(jnp.broadcast_to(shift_ref[...], (DK, ROWS)))
    log_decay = jnp.log(forget) + shift
    lower = jnp.where(iota((ROWS, ROWS), 0) >= iota((ROWS, ROWS), 1), 1.0, 0.0)
    running = mm(lower, log_decay, HIGH)
    values = v_ref[...].astype(F32)
    query = q_ref[...].astype(F32)
    closing = running[ROWS - 1:ROWS, :]
    values_t = jnp.transpose(values)
    state_t = mm(values_t, keys * jnp.exp(closing - running), HIGH)
    sx[x, 0:DK, :] = state_t.astype(BF16)
    sx[x, DK:PACK, :] = jnp.broadcast_to(jnp.exp(closing), (PACK - DK, DK)).astype(BF16)
    for dx in range(1, NX):
        push(sx.at[x], sx.at[x], xsend.at[dx], xrecv.at[dx],
             (z, lax.rem(x + dx, NX), y, c))

    causal = iota((SUB, SUB), 0) >= iota((SUB, SUB), 1)
    local = []
    for i in range(ROWS // SUB):
        lo, hi = i * SUB, (i + 1) * SUB
        decay_i, query_i = running[lo:hi], query[lo:hi]
        middle = running[lo + SUB // 2 - 1:lo + SUB // 2]
        scores = jnp.where(causal, nt_dot(
            query_i * jnp.exp(decay_i - middle), keys[lo:hi] * jnp.exp(middle - decay_i),
            HIGH), 0.0)
        out = mm(scores, values[lo:hi], HIGH)
        if i:
            start = running[lo - 1:lo]
            scores = nt_dot(query_i * jnp.exp(decay_i - start),
                            keys[:lo] * jnp.exp(start - running[:lo]), HIGH)
            out = out + mm(scores, values[:lo], HIGH)
        local.append(out)
    qd_v[0] = jnp.concatenate(local, axis=0)
    qd_v[1] = query * jnp.exp(running)

    slot0 = (e0 * RBLK + rank0).astype(F32)
    slot1 = (e1 * RBLK + rank1).astype(F32)
    which = iota((DK, ROWS), 0)
    table = jnp.where(which == 0, slot0, jnp.where(which == 1, slot1, jnp.where(
        which == 2, rw_ref[0:1, :], jnp.where(which == 3, rw_ref[1:2, :], 0.0))))
    table = jnp.transpose(table)
    place0, place1 = table[:, 0:1].astype(I32), table[:, 1:2].astype(I32)
    for g in range(4):
        spot = iota((ROWS, 256), 1) + 256 * g
        weight = jnp.where(spot == place0, table[:, 2:3], 0.0) + jnp.where(
            spot == place1, table[:, 3:4], 0.0)
        high = weight.astype(BF16)
        qh_v[:, 256 * g:256 * g + 256] = high
        ql_v[:, 256 * g:256 * g + 256] = (weight - high.astype(F32)).astype(BF16)

    for o in SEND_ORDER:
        source = lax.rem(me + N_EP - 2 * o + N_EP - c, N_EP)
        if o:
            await_in(rbuf.at[lax.div(source, 2)], dsend.at[o], drecv.at[o])
        else:
            @pl.when(c == 1)
            def _():
                await_in(rbuf.at[lax.div(source, 2)], dsend.at[0], drecv.at[0])

            @pl.when(c == 0)
            def _():
                own_copy.wait()
    row, col = iota((4 * CAP, 4 * DBLK), 0), iota((4 * CAP, 4 * DBLK), 1)
    spot = row + (DBLK - CAP) * ((row * 3277) >> 16)
    packs = [ones_where(col == spot + CAP * h) for h in range(2)]
    for g in range(4):
        block = rbuf[4 * g:4 * g + 4].reshape(4 * DBLK, DK)
        for h in range(2):
            xs[y, c, g // 2, (g % 2) * 80:(g % 2) * 80 + 80, h * DK:(h + 1) * DK] = mm(
                packs[h], block).astype(BF16)

    def slab(j):
        return lax.rem(y + j, NY)

    def ring_send(buf, direction, hop, sub, send, recv):
        j = (NY - hop) % NY if direction == 0 else hop
        index = direction * 8 + hop * 2 + sub
        push(buf.at[slab(j), c, sub], buf.at[slab(j), c, sub], send.at[index], recv.at[index],
             up if direction == 0 else down)

    def ring_take(buf, direction, hop, sub, send, recv):
        j = (NY - hop) % NY if direction == 0 else hop
        index = direction * 8 + (hop - 1) * 2 + sub
        await_in(buf.at[slab(j), c, sub], send.at[index], recv.at[index])
        return j

    def pair_send(buf, j, sub, send, recv):
        push(buf.at[slab(j), c, sub], buf.at[slab(j), c, sub],
             send.at[2 * j + sub], recv.at[2 * j + sub], partner)

    def pair_take(buf, j, sub, send, recv):
        await_in(buf.at[slab(j), 1 - c, sub], send.at[2 * j + sub], recv.at[2 * j + sub])

    far, near = ((0, 0), (1, 1)), ((0, 1), (1, 0))

    def gather_start(buf, send, recv, psend, precv):
        for direction, sub in far + near:
            ring_send(buf, direction, 0, sub, send, recv)
        for sub in range(2):
            pair_send(buf, 0, sub, psend, precv)

    def gather_hop(buf, hop, send, recv, psend, precv):
        for direction, sub in far + (near if hop < 4 else ()):
            j = ring_take(buf, direction, hop, sub, send, recv)
            if hop < (4 if (direction, sub) in far else 3):
                ring_send(buf, direction, hop, sub, send, recv)
            pair_send(buf, j, sub, psend, precv)

    gather_start(xs, asend, arecv, psend, precv)

    def read_state(ref, k):
        return ref[k, DK:PACK, :].astype(F32)[0:1], ref[k, 0:DK, :].astype(F32)

    def step(before, after):
        return before[0] * after[0], after[0] * before[1] + after[1]

    def prefix(ref, count, index):
        running = (jnp.ones((1, DK), F32), jnp.zeros((DK, DK), F32))
        inside = running
        for k in range(count):
            running = step(running, read_state(ref, k))
            inside = tuple(jnp.where(k < index, a, b) for a, b in zip(running, inside))
        return inside, running

    for dx in range(1, NX):
        await_in(sx.at[lax.rem(x + NX - dx, NX)], xsend.at[dx], xrecv.at[dx])
    inside_x, whole = prefix(sx, NX, x)
    sz[z, 0:DK, :] = whole[1].astype(BF16)
    sz[z, DK:PACK, :] = jnp.broadcast_to(whole[0], (PACK - DK, DK)).astype(BF16)
    for dz in (4, 3, 5, 2, 6, 1, 7):
        push(sz.at[z], sz.at[z], zsend.at[dz], zrecv.at[dz],
             (lax.rem(z + dz, NZ), x, y, c))

    weights_in[0].wait()
    weights_in[1].wait()

    def expert_in(j, first=False):
        for sub in range(2):
            pair_take(xs, j, sub, psend, precv)
        rows = xs[slab(j)].reshape(SLOTS, FPD)
        depth = pl.ds(pl.multiple_of(slab(j) * FPD, FPD), FPD)
        if first:
            accg[...] = mm(rows, wg_v[depth, :])
            accu[...] = mm(rows, wu_v[depth, :])
        else:
            accg[...] += mm(rows, wg_v[depth, :])
            accu[...] += mm(rows, wu_v[depth, :])

    gather_hop(xs, 1, asend, arecv, psend, precv)
    expert_in(0, True)
    gather_hop(xs, 2, asend, arecv, psend, precv)
    expert_in(1)
    expert_in(7)

    for dz in range(1, NZ):
        await_in(sz.at[lax.rem(z + NZ - dz, NZ)], zsend.at[dz], zrecv.at[dz])
    before, _ = prefix(sz, NZ, z)
    incoming = step(before, inside_x)[1]
    result = qd_v[0] + nt_dot(qd_v[1], incoming, HIGH)
    inverse = lax.rsqrt(jnp.mean(result * result, axis=1, keepdims=True) + EPS)
    head_out = result * inverse * hgain_ref[...] * jax.nn.silu(og_ref[...].astype(F32))
    hs[y, c] = head_out.astype(BF16).reshape(2, ROWS // 2, DK)

    gather_hop(xs, 3, asend, arecv, psend, precv)
    expert_in(2)
    expert_in(6)
    gather_hop(xs, 4, asend, arecv, psend, precv)
    expert_in(3)
    expert_in(5)
    expert_in(4)

    for i in range(4):
        block = slice(160 * i, 160 * i + 160)
        hid[block, :] = (jax.nn.silu(accg[block, :]) * accu[block, :]).astype(BF16)
    for copy in weights_in[3:]:
        copy.wait()

    def expert_out(j):
        partial = mm(hid[...], wd_v[slab(j)]).astype(BF16)
        part[j] = partial[:, :DK]
        pout[j] = partial[:, DK:]
        push(pout.at[j], pin.at[j], csend.at[j], crecv.at[j], partner)

    def chip_sum(j, sub):
        block = slice(HALF * sub, HALF * sub + HALF)
        return part[j, block, :].astype(F32) + pin[j, block, :].astype(F32)

    def sum_send(direction, step, sub, value):
        index = direction * 8 + step * 2 + sub
        rsend[direction, step, sub] = value.astype(BF16)
        push(rsend.at[direction, step, sub], rrecv.at[direction, step, sub],
             ssend.at[index], srecv.at[index], up if direction == 0 else down)

    def sum_take(direction, step, sub):
        index = direction * 8 + step * 2 + sub
        await_in(rrecv.at[direction, step, sub], ssend.at[index], srecv.at[index])
        return rrecv[direction, step, sub].astype(F32)

    def ready(j):
        await_in(pin.at[j], csend.at[j], crecv.at[j])

    def target(direction, sub, step):
        j = (4 if (direction, sub) in far else 3) - step
        return j % NY if direction == 0 else -j % NY

    for j in (4, 3, 5):
        expert_out(j)
    ready(4)
    for direction, sub in far:
        sum_send(direction, 0, sub, chip_sum(target(direction, sub, 0), sub))
    ready(3)
    ready(5)
    for direction, sub in near:
        sum_send(direction, 0, sub, chip_sum(target(direction, sub, 0), sub))
    for j in (2, 6, 1, 7, 0):
        expert_out(j)
    last = {}
    for step_at in range(1, 5):
        if step_at == 1:
            late = (2, 6)
        elif step_at == 2:
            late = (1, 7)
        elif step_at == 3:
            late = (0,)
        else:
            late = ()
        for direction, sub in far:
            if step_at < 4:
                value = sum_take(direction, step_at - 1, sub)
                sum_send(direction, step_at, sub,
                         value + chip_sum(target(direction, sub, step_at), sub))
        for j in late:
            ready(j)
        for direction, sub in near:
            if step_at < 3:
                value = sum_take(direction, step_at - 1, sub)
                sum_send(direction, step_at, sub,
                         value + chip_sum(target(direction, sub, step_at), sub))
    for direction, sub in near:
        last[sub] = chip_sum(0, sub) + sum_take(direction, 2, sub)
    for direction, sub in far:
        last[sub] = last[sub] + sum_take(direction, 3, sub)

    row, col = iota((4 * RBLK, 4 * CAP), 0), iota((4 * RBLK, 4 * CAP), 1)
    spread = ones_where((col == (row >> 5) * CAP + (row & 31)) & ((row & 31) < CAP))
    for g in range(8):
        value = last[g // 4][(g % 4) * 80:(g % 4) * 80 + 80].astype(BF16)
        rout[4 * g:4 * g + 4] = mm(spread, value).astype(BF16).reshape(4, RBLK, DK)
    for o in RETURN_ORDER:
        there = lax.rem(me + o, N_EP)
        push(rout.at[lax.rem(there + x, 2) * 16 + lax.div(there, 2)], rin.at[me],
             bsend.at[o], brecv.at[o], at_ep(there))
    rin[me] = rout[lax.div(me, 2)]

    gather_start(hs, hsend, hrecv, gsend, grecv)
    weights_in[2].wait()

    def project(j):
        for sub in range(2):
            pair_take(hs, j, sub, gsend, grecv)
        heads = hs[slab(j)].reshape(2, ROWS, DK)
        rows = jnp.concatenate([heads[0], heads[1]], axis=1)
        return mm(rows, wmix_v[pl.ds(pl.multiple_of(slab(j) * FPD, FPD), FPD), :])

    gather_hop(hs, 1, hsend, hrecv, gsend, grecv)
    mixed = project(0)
    gather_hop(hs, 2, hsend, hrecv, gsend, grecv)
    mixed += project(1) + project(7)
    gather_hop(hs, 3, hsend, hrecv, gsend, grecv)
    mixed += project(2) + project(6)
    gather_hop(hs, 4, hsend, hrecv, gsend, grecv)
    mixed += project(3) + project(5)
    mixed += project(4)
    mixed_ref[...] = mixed.astype(BF16)

    for o in RETURN_ORDER:
        await_in(rin.at[lax.rem(me + N_EP - o, N_EP)], bsend.at[o], brecv.at[o])
    returned = rin[...].reshape(N_EP * RBLK, DK)
    moe_ref[...] = (mm(qh_v[...], returned) + mm(ql_v[...], returned)).astype(BF16)

    for copy in pending:
        copy.wait_send()
    for o in SEND_ORDER:
        if o:
            dispatch(o).wait_send()
        else:
            @pl.when(c == 1)
            def _():
                dispatch(0).wait_send()


def body(
    mix_query, forget_input, mix_value, out_gate_input, decay_shift, forget_floor, head_gain,
    w_mix_out, moe_input, moe_gain, routes, route_weight, w_exp_gate, w_exp_up, w_exp_down,
):
    vmem = pl.BlockSpec(memory_space=pltpu.VMEM)
    hbm = pl.BlockSpec(memory_space=pl.ANY)
    sem = pltpu.SemaphoreType.DMA
    outs = jax.ShapeDtypeStruct((ROWS, DK), BF16)
    return pl.pallas_call(
        kernel,
        out_shape=(outs, outs),
        in_specs=[vmem] * 7 + [hbm] * 2 + [vmem] * 3 + [hbm] * 3,
        out_specs=(vmem, vmem),
        scratch_shapes=[
            pltpu.VMEM((ROWS, D), BF16),
            pltpu.VMEM((ROWS, FPD), BF16),
            pltpu.VMEM((D, FPD), BF16),
            pltpu.VMEM((D, FPD), BF16),
            pltpu.VMEM((NY, FPD, FPD), BF16),
            pltpu.VMEM((D, DK), BF16),
            pltpu.VMEM((ROWS, FPD), BF16),
            pltpu.VMEM((16, DBLK, DK), BF16),
            pltpu.VMEM((16, DBLK, DK), BF16),
            pltpu.VMEM((NY, 2, 2, HALF // 2, FPD), BF16),
            pltpu.VMEM((SLOTS, FPD), F32),
            pltpu.VMEM((SLOTS, FPD), F32),
            pltpu.VMEM((SLOTS, FPD), BF16),
            pltpu.VMEM((NY, SLOTS, DK), BF16),
            pltpu.VMEM((NY, SLOTS, DK), BF16),
            pltpu.VMEM((NY, SLOTS, DK), BF16),
            pltpu.VMEM((2, 4, 2, HALF, DK), BF16),
            pltpu.VMEM((2, 4, 2, HALF, DK), BF16),
            pltpu.VMEM((N_EP, RBLK, DK), BF16),
            pltpu.VMEM((N_EP, RBLK, DK), BF16),
            pltpu.VMEM((ROWS, N_EP * RBLK), BF16),
            pltpu.VMEM((ROWS, N_EP * RBLK), BF16),
            pltpu.VMEM((NX, PACK, DK), BF16),
            pltpu.VMEM((NZ, PACK, DK), BF16),
            pltpu.VMEM((2, ROWS, DK), F32),
            pltpu.VMEM((NY, 2, 2, ROWS // 2, DK), BF16),
            sem((6,)), sem((19,)), sem((16,)), sem((16,)), sem((16,)), sem((16,)),
            sem((16,)), sem((16,)), sem((8,)), sem((8,)), sem((16,)), sem((16,)),
            sem((N_EP,)), sem((N_EP,)), sem((NX,)), sem((NX,)), sem((NZ,)), sem((NZ,)),
            sem((16,)), sem((16,)), sem((16,)), sem((16,)),
        ],
        compiler_params=pltpu.CompilerParams(collective_id=0, has_side_effects=True),
        name="step",
    )(
        mix_query, forget_input, mix_value, out_gate_input,
        decay_shift.reshape(1, ROWS), forget_floor.reshape(1, DK), head_gain.reshape(1, DK),
        w_mix_out, moe_input, moe_gain.reshape(NY, FPD), routes.T, route_weight.T,
        w_exp_gate[0], w_exp_up[0], w_exp_down[0],
    )


def solution(mesh):
    torus = Mesh(mesh.devices.reshape(NZ, NX, NY, 2), ("ep_0", "ep_1", "tp_0", "tp_1"))
    placed = (
        P(EP, TP), P(EP, TP), P(EP, TP), P(EP, TP), P(EP, TP), P(TP), P(), P(None, TP),
        P(EP, None), P(), P(EP, None), P(EP, None), P(EP, None, TP), P(EP, None, TP),
        P(EP, TP, None),
    )
    return jax.shard_map(
        body, mesh=torus, in_specs=placed, out_specs=(P(EP, TP), P(EP, TP)), check_vma=False
    )
```

```python
import jax
import jax.numpy as jnp
from jax import lax
from jax.experimental import pallas as pl
from jax.experimental.pallas import tpu as pltpu
from jax.sharding import Mesh
from jax.sharding import PartitionSpec as P

EP = ("ep_0", "ep_1")
TP = ("tp_0", "tp_1")
NZ, NX, NY = 8, 4, 8
N_EP = NZ * NX
ROWS = 256
CAP = 20
D = 2048
DK = 128
FPD = 256
HALF = CAP * N_EP // 2
SLOTS = CAP * N_EP
DBLK = 40
RBLK = 24
SUB = 64
PACK = DK + 16
EPS = 1e-6
MESH = pl.DeviceIdType.MESH
F32 = jnp.float32
BF16 = jnp.bfloat16
I32 = jnp.int32
HIGH = lax.Precision.HIGHEST

SEND_ORDER = (8, 7, 9, 6, 10, 5, 11, 4, 12, 3, 13, 2, 14, 1, 15, 0)
RETURN_ORDER = sorted(range(1, N_EP), key=lambda o: -min(o, N_EP - o))
CHUNK_ORDER = (4, 3, 5, 2, 6, 1, 7, 0)


def ones_where(mask):
    return jnp.where(mask, 1.0, 0.0).astype(BF16)


def nt_dot(a, b, precision=None):
    return lax.dot_general(
        a, b, (((1,), (1,)), ((), ())), precision=precision, preferred_element_type=F32
    )


def mm(a, b, precision=None):
    return jnp.dot(a, b, precision=precision, preferred_element_type=F32)


def iota(shape, dim):
    return lax.broadcasted_iota(I32, shape, dim)


def kernel(
    q_hbm, f_hbm, v_hbm, og_hbm, shift_ref, floor_ref, hgain_ref, wmix_hbm,
    moe_hbm, gain_ref, routes_ref, rw_ref, wg_hbm, wu_hbm, wd_hbm,
    mixed_ref, moe_ref,
    mixer_v, moe_v, mine_v, wg_v, wu_v, wd_v, wmix_v, norm_v,
    sbuf, rbuf, xs, accg, accu, hid, part, pout, pin, rsend, rrecv,
    rout, rin, qh_v, ql_v, sx, sz, qd_v, hs,
    lsem, wsem, dsend, drecv, asend, arecv, psend, precv, csend, crecv,
    ssend, srecv, bsend, brecv, xsend, xrecv, zsend, zrecv, hsend, hrecv,
    gsend, grecv,
):
    z = lax.axis_index("ep_0")
    x = lax.axis_index("ep_1")
    y = lax.axis_index("tp_0")
    c = lax.axis_index("tp_1")
    me = z * NX + x

    def at_ep(e):
        return (lax.div(e, NX), lax.rem(e, NX), y, c)

    up = (z, x, lax.rem(y + 1, NY), c)
    down = (z, x, lax.rem(y + NY - 1, NY), c)
    partner = (z, x, y, 1 - c)

    def remote(src, dst, send, recv, device):
        return pltpu.make_async_remote_copy(
            src_ref=src, dst_ref=dst, send_sem=send, recv_sem=recv,
            device_id=device, device_id_type=MESH,
        )

    pending = []

    def push(src, dst, send, recv, device):
        copy = remote(src, dst, send, recv, device)
        copy.start()
        pending.append(copy)

    def await_in(dst, send, recv):
        remote(dst, dst, send, recv, partner).wait_recv()

    rows_in = []
    for i in range(4):
        rows_in.append(pltpu.make_async_copy(
            moe_hbm.at[pl.ds(64 * i, 64), :], moe_v.at[pl.ds(64 * i, 64), :], lsem.at[i]))
    rows_in.append(pltpu.make_async_copy(
        moe_hbm.at[:, pl.ds(pl.multiple_of(y * FPD, FPD), FPD)], mine_v.at[0], lsem.at[4]))
    rows_in.append(pltpu.make_async_copy(
        moe_hbm.at[:, pl.ds(pl.multiple_of(lax.rem(y + NY // 2, NY) * FPD, FPD), FPD)],
        mine_v.at[1], lsem.at[6]))
    for copy in rows_in:
        copy.start()
    mixer_in = [
        pltpu.make_async_copy(ref, mixer_v.at[i], lsem.at[7 + i])
        for i, ref in enumerate((f_hbm, v_hbm, q_hbm, og_hbm))]
    for copy in mixer_in:
        copy.start()

    barrier = pltpu.get_barrier_semaphore()

    def greet(o, carry):
        pl.semaphore_signal(
            barrier, inc=1, device_id=at_ep(lax.rem(me + o, N_EP)), device_id_type=MESH)
        return carry

    lax.fori_loop(1, N_EP, greet, 0)
    for device in (up, down, partner):
        pl.semaphore_signal(barrier, inc=1, device_id=device, device_id_type=MESH)

    weights_in = [
        pltpu.make_async_copy(wg_hbm, wg_v, wsem.at[0]),
        pltpu.make_async_copy(wu_hbm, wu_v, wsem.at[1]),
        pltpu.make_async_copy(wmix_hbm, wmix_v, wsem.at[2]),
    ]
    for i in range(NY):
        for h in range(2):
            column = pl.multiple_of(i * FPD + lax.rem(c + h, 2) * DK, DK)
            weights_in.append(pltpu.make_async_copy(
                wd_hbm.at[:, pl.ds(column, DK)],
                wd_v.at[i, :, pl.ds(h * DK, DK)], wsem.at[3 + 2 * i + h]))
    for copy in weights_in:
        copy.start()

    e0, e1 = routes_ref[0:1, :], routes_ref[1:2, :]
    ids = iota((N_EP, ROWS), 0)
    one0, one1 = ids == e0, ids == e1
    ones = jnp.concatenate([ones_where(one0), ones_where(one1)], axis=0)
    strict = ones_where(iota((ROWS, ROWS), 0) < iota((ROWS, ROWS), 1))
    earlier = mm(ones, strict)
    total0 = jnp.sum(jnp.where(one0, 1.0, 0.0), axis=1, keepdims=True)
    rank0 = jnp.sum(jnp.where(one0, earlier[:N_EP], 0.0), axis=0, keepdims=True).astype(I32)
    rank1 = jnp.sum(
        jnp.where(one1, earlier[N_EP:] + total0, 0.0), axis=0, keepdims=True).astype(I32)

    for i in range(4):
        rows_in[i].wait()
    rows_in[4].wait()
    rows_in[5].wait()
    halves = (y, lax.rem(y + NY // 2, NY))
    gains = [gain_ref[:, pl.ds(pl.multiple_of(k * FPD, FPD), FPD)] for k in halves]
    for i in range(4):
        block = moe_v[64 * i:64 * i + 64, :].astype(F32)
        mean = jnp.sum(block * block, axis=1, keepdims=True) * (1.0 / D)
        for k in range(2):
            own = mine_v[k, 64 * i:64 * i + 64, :].astype(F32)
            norm_v[k, 64 * i:64 * i + 64, :] = (
                own * lax.rsqrt(mean + EPS) * gains[k]).astype(BF16)

    parity = lax.rem(x + c, 2)
    target0 = jnp.where((e0 & 1) == parity, (e0 >> 1) * DBLK + rank0, -1000)
    target1 = jnp.where((e1 & 1) == parity, (e1 >> 1) * DBLK + rank1, -1000)
    n0 = jnp.concatenate([norm_v[0, :, :DK], norm_v[1, :, :DK]], axis=1)
    n1 = jnp.concatenate([norm_v[0, :, DK:], norm_v[1, :, DK:]], axis=1)
    for g in range(4):
        spot = iota((4 * DBLK, ROWS), 0) + 4 * DBLK * g
        first = ones_where((spot == target0) | (spot == target1))
        second = ones_where((spot == target0 + CAP) | (spot == target1 + CAP))
        rows = (mm(first, n0) + mm(second, n1)).astype(BF16)
        for k in range(2):
            sbuf[k, 4 * g:4 * g + 4] = rows[:, k * DK:(k + 1) * DK].reshape(4, DBLK, DK)

    pl.semaphore_wait(barrier, N_EP + 2)

    def dispatch(k, o):
        expert = lax.rem(me + 2 * o + c, N_EP)
        return remote(sbuf.at[k, lax.div(expert, 2)], rbuf.at[k, lax.div(me, 2)],
                      dsend.at[16 * k + o], drecv.at[16 * k + o], at_ep(expert))

    own_copies = [pltpu.make_async_copy(
        sbuf.at[k, lax.div(me, 2)], rbuf.at[k, lax.div(me, 2)], lsem.at[k * 6 + 5])
        for k in range(2)]
    for k in range(2):
        for o in SEND_ORDER:
            if o:
                dispatch(k, o).start()
            else:
                @pl.when(c == 1)
                def _():
                    dispatch(k, 0).start()

                @pl.when(c == 0)
                def _():
                    own_copies[k].start()

    floor = floor_ref[...]
    for copy in mixer_in:
        copy.wait()
    pre = mixer_v[0].astype(F32)
    forget = floor + (1.0 - floor) * jax.nn.sigmoid(pre)
    keys = (1.0 - floor) * jax.nn.sigmoid(-pre)
    shift = jnp.transpose(jnp.broadcast_to(shift_ref[...], (DK, ROWS)))
    log_decay = jnp.log(forget) + shift
    lower = jnp.where(iota((ROWS, ROWS), 0) >= iota((ROWS, ROWS), 1), 1.0, 0.0)
    running = mm(lower, log_decay, HIGH)
    values = mixer_v[1].astype(F32)
    query = mixer_v[2].astype(F32)
    closing = running[ROWS - 1:ROWS, :]
    values_t = jnp.transpose(values)
    state_t = mm(values_t, keys * jnp.exp(closing - running), HIGH)
    sx[x, 0:DK, :] = state_t.astype(BF16)
    sx[x, DK:PACK, :] = jnp.broadcast_to(jnp.exp(closing), (PACK - DK, DK)).astype(BF16)
    for dx in range(1, NX):
        push(sx.at[x], sx.at[x], xsend.at[dx], xrecv.at[dx],
             (z, lax.rem(x + dx, NX), y, c))

    def arrived(k):
        for o in SEND_ORDER:
            source = lax.rem(me + N_EP - 2 * o + N_EP - c, N_EP)
            slot = rbuf.at[k, lax.div(source, 2)]
            if o:
                await_in(slot, dsend.at[16 * k + o], drecv.at[16 * k + o])
            else:
                @pl.when(c == 1)
                def _():
                    await_in(slot, dsend.at[16 * k], drecv.at[16 * k])

                @pl.when(c == 0)
                def _():
                    own_copies[k].wait()

    row, col = iota((4 * CAP, 4 * DBLK), 0), iota((4 * CAP, 4 * DBLK), 1)
    spot = row + (DBLK - CAP) * ((row * 3277) >> 16)
    packs = [ones_where(col == spot + CAP * h) for h in range(2)]

    def pack(k):
        arrived(k)
        for g in range(4):
            block = rbuf[k, 4 * g:4 * g + 4].reshape(4 * DBLK, DK)
            for h in range(2):
                xs[halves[k], c, g // 2, (g % 2) * 80:(g % 2) * 80 + 80,
                   h * DK:(h + 1) * DK] = mm(packs[h], block).astype(BF16)

    pack(0)

    def slab(j):
        return lax.rem(y + j, NY)

    def ring_send(buf, direction, hop, sub, send, recv):
        j = (NY - hop) % NY if direction == 0 else hop
        index = direction * 8 + hop * 2 + sub
        push(buf.at[slab(j), c, sub], buf.at[slab(j), c, sub], send.at[index], recv.at[index],
             up if direction == 0 else down)

    def ring_take(buf, direction, hop, sub, send, recv):
        j = (NY - hop) % NY if direction == 0 else hop
        index = direction * 8 + (hop - 1) * 2 + sub
        await_in(buf.at[slab(j), c, sub], send.at[index], recv.at[index])
        return j

    def pair_send(buf, j, sub, send, recv):
        push(buf.at[slab(j), c, sub], buf.at[slab(j), c, sub],
             send.at[2 * j + sub], recv.at[2 * j + sub], partner)

    def pair_take(buf, j, sub, send, recv):
        await_in(buf.at[slab(j), 1 - c, sub], send.at[2 * j + sub], recv.at[2 * j + sub])

    far, near = ((0, 0), (1, 1)), ((0, 1), (1, 0))

    def gather_start(buf, send, recv, psend, precv):
        for direction, sub in far + near:
            ring_send(buf, direction, 0, sub, send, recv)
        for sub in range(2):
            pair_send(buf, 0, sub, psend, precv)

    def gather_hop(buf, hop, send, recv, psend, precv):
        for direction, sub in far + (near if hop < 4 else ()):
            j = ring_take(buf, direction, hop, sub, send, recv)
            if hop < (4 if (direction, sub) in far else 3):
                ring_send(buf, direction, hop, sub, send, recv)
            pair_send(buf, j, sub, psend, precv)

    for sub in range(2):
        for direction in range(2):
            ring_send(xs, direction, 0, sub, asend, arecv)
        pair_send(xs, 0, sub, psend, precv)

    def rows_hop(hop, sub):
        for direction in range(2):
            j = ring_take(xs, direction, hop, sub, asend, arecv)
            if hop < 3:
                ring_send(xs, direction, hop, sub, asend, arecv)
            pair_send(xs, j, sub, psend, precv)


    def read_state(ref, k):
        return ref[k, DK:PACK, :].astype(F32)[0:1], ref[k, 0:DK, :].astype(F32)

    def step(before, after):
        return before[0] * after[0], after[0] * before[1] + after[1]

    def prefix(ref, count, index):
        running = (jnp.ones((1, DK), F32), jnp.zeros((DK, DK), F32))
        inside = running
        for k in range(count):
            running = step(running, read_state(ref, k))
            inside = tuple(jnp.where(k < index, a, b) for a, b in zip(running, inside))
        return inside, running

    for dx in range(1, NX):
        await_in(sx.at[lax.rem(x + NX - dx, NX)], xsend.at[dx], xrecv.at[dx])
    inside_x, whole = prefix(sx, NX, x)
    sz[z, 0:DK, :] = whole[1].astype(BF16)
    sz[z, DK:PACK, :] = jnp.broadcast_to(whole[0], (PACK - DK, DK)).astype(BF16)

    def along_z(dz):
        return remote(sz.at[z], sz.at[z], zsend.at[dz], zrecv.at[dz],
                      (lax.rem(z + dz, NZ), x, y, c))

    for dz in range(1, NZ):
        @pl.when(z + dz < NZ)
        def _():
            along_z(dz).start()

    causal = iota((SUB, SUB), 0) >= iota((SUB, SUB), 1)
    local = []
    for i in range(ROWS // SUB):
        lo, hi = i * SUB, (i + 1) * SUB
        decay_i, query_i = running[lo:hi], query[lo:hi]
        middle = running[lo + SUB // 2 - 1:lo + SUB // 2]
        scores = jnp.where(causal, nt_dot(
            query_i * jnp.exp(decay_i - middle), keys[lo:hi] * jnp.exp(middle - decay_i),
            HIGH), 0.0)
        out = mm(scores, values[lo:hi], HIGH)
        if i:
            start = running[lo - 1:lo]
            scores = nt_dot(query_i * jnp.exp(decay_i - start),
                            keys[:lo] * jnp.exp(start - running[:lo]), HIGH)
            out = out + mm(scores, values[:lo], HIGH)
        local.append(out)
    qd_v[0] = jnp.concatenate(local, axis=0)
    qd_v[1] = query * jnp.exp(running)


    weights_in[0].wait()
    weights_in[1].wait()

    def expert_in(j, first=False):
        for sub in range(2):
            pair_take(xs, j, sub, psend, precv)
        rows = xs[slab(j)].reshape(SLOTS, FPD)
        depth = pl.ds(pl.multiple_of(slab(j) * FPD, FPD), FPD)
        if first:
            accg[...] = mm(rows, wg_v[depth, :])
            accu[...] = mm(rows, wu_v[depth, :])
        else:
            accg[...] += mm(rows, wg_v[depth, :])
            accu[...] += mm(rows, wu_v[depth, :])

    rows_hop(1, 0)
    rows_hop(1, 1)
    expert_in(0, True)
    rows_hop(2, 0)
    expert_in(1)
    rows_hop(2, 1)
    expert_in(7)
    pack(1)
    for sub in range(2):
        pair_send(xs, 4, sub, psend, precv)

    slot0 = (e0 * RBLK + rank0).astype(F32)
    slot1 = (e1 * RBLK + rank1).astype(F32)
    which = iota((DK, ROWS), 0)
    table = jnp.where(which == 0, slot0, jnp.where(which == 1, slot1, jnp.where(
        which == 2, rw_ref[0:1, :], jnp.where(which == 3, rw_ref[1:2, :], 0.0))))
    table = jnp.transpose(table)
    place0, place1 = table[:, 0:1].astype(I32), table[:, 1:2].astype(I32)
    for g in range(N_EP * RBLK // 256):
        spot = iota((ROWS, 256), 1) + 256 * g
        weight = jnp.where(spot == place0, table[:, 2:3], 0.0) + jnp.where(
            spot == place1, table[:, 3:4], 0.0)
        high = weight.astype(BF16)
        qh_v[:, 256 * g:256 * g + 256] = high
        ql_v[:, 256 * g:256 * g + 256] = (weight - high.astype(F32)).astype(BF16)

    rows_hop(3, 0)
    expert_in(2)
    expert_in(6)
    expert_in(4)

    for dz in range(1, NZ):
        @pl.when(z >= dz)
        def _():
            await_in(sz.at[lax.rem(z + NZ - dz, NZ)], zsend.at[dz], zrecv.at[dz])

    before, _ = prefix(sz, NZ, z)
    incoming = step(before, inside_x)[1]
    result = qd_v[0] + nt_dot(qd_v[1], incoming, HIGH)
    inverse = lax.rsqrt(jnp.mean(result * result, axis=1, keepdims=True) + EPS)
    head_out = result * inverse * hgain_ref[...] * jax.nn.silu(mixer_v[3].astype(F32))
    hs[y, c] = head_out.astype(BF16).reshape(2, ROWS // 2, DK)

    gather_start(hs, hsend, hrecv, gsend, grecv)
    rows_hop(3, 1)
    expert_in(3)
    expert_in(5)

    for i in range(4):
        block = slice(160 * i, 160 * i + 160)
        hid[block, :] = (jax.nn.silu(accg[block, :]) * accu[block, :]).astype(BF16)
    for copy in weights_in[3:]:
        copy.wait()

    def expert_out(j):
        partial = mm(hid[...], wd_v[slab(j)]).astype(BF16)
        part[j] = partial[:, :DK]
        pout[j] = partial[:, DK:]
        push(pout.at[j], pin.at[j], csend.at[j], crecv.at[j], partner)

    def chip_sum(j, sub):
        block = slice(HALF * sub, HALF * sub + HALF)
        return part[j, block, :].astype(F32) + pin[j, block, :].astype(F32)

    def sum_send(direction, step, sub, value):
        index = direction * 8 + step * 2 + sub
        rsend[direction, step, sub] = value.astype(BF16)
        push(rsend.at[direction, step, sub], rrecv.at[direction, step, sub],
             ssend.at[index], srecv.at[index], up if direction == 0 else down)

    def sum_take(direction, step, sub):
        index = direction * 8 + step * 2 + sub
        await_in(rrecv.at[direction, step, sub], ssend.at[index], srecv.at[index])
        return rrecv[direction, step, sub].astype(F32)

    def ready(j):
        await_in(pin.at[j], csend.at[j], crecv.at[j])

    def target(direction, sub, step):
        j = (4 if (direction, sub) in far else 3) - step
        return j % NY if direction == 0 else -j % NY

    for j in (4, 3, 5):
        expert_out(j)
    gather_hop(hs, 1, hsend, hrecv, gsend, grecv)
    ready(4)
    for direction, sub in far:
        sum_send(direction, 0, sub, chip_sum(target(direction, sub, 0), sub))
    ready(3)
    ready(5)
    for direction, sub in near:
        sum_send(direction, 0, sub, chip_sum(target(direction, sub, 0), sub))
    for j in (2, 6):
        expert_out(j)
    gather_hop(hs, 2, hsend, hrecv, gsend, grecv)
    for j in (1, 7, 0):
        expert_out(j)
    weights_in[2].wait()

    def project(j):
        for sub in range(2):
            pair_take(hs, j, sub, gsend, grecv)
        heads = hs[slab(j)].reshape(2, ROWS, DK)
        rows = jnp.concatenate([heads[0], heads[1]], axis=1)
        return mm(rows, wmix_v[pl.ds(pl.multiple_of(slab(j) * FPD, FPD), FPD), :])

    last = {}
    for step_at in range(1, 5):
        if step_at == 1:
            late = (2, 6)
        elif step_at == 2:
            late = (1, 7)
        elif step_at == 3:
            late = (0,)
        else:
            late = ()
            mixed += project(1) + project(7) + project(2) + project(6)
        for direction, sub in far:
            if step_at < 4:
                value = sum_take(direction, step_at - 1, sub)
                sum_send(direction, step_at, sub,
                         value + chip_sum(target(direction, sub, step_at), sub))
        for j in late:
            ready(j)
        for direction, sub in near:
            if step_at < 3:
                value = sum_take(direction, step_at - 1, sub)
                sum_send(direction, step_at, sub,
                         value + chip_sum(target(direction, sub, step_at), sub))
        if step_at == 1:
            gather_hop(hs, 3, hsend, hrecv, gsend, grecv)
            mixed = project(0)
        elif step_at == 2:
            gather_hop(hs, 4, hsend, hrecv, gsend, grecv)
    for direction, sub in near:
        last[sub] = chip_sum(0, sub) + sum_take(direction, 2, sub)
    for direction, sub in far:
        last[sub] = last[sub] + sum_take(direction, 3, sub)

    row, col = iota((4 * RBLK, 4 * CAP), 0), iota((4 * RBLK, 4 * CAP), 1)
    group = (row * 2731) >> 16
    spread = ones_where((col == row - (RBLK - CAP) * group) & (row - RBLK * group < CAP))
    for g in range(8):
        value = last[g // 4][(g % 4) * 80:(g % 4) * 80 + 80].astype(BF16)
        rout[4 * g:4 * g + 4] = mm(spread, value).astype(BF16).reshape(4, RBLK, DK)
    for o in RETURN_ORDER:
        there = lax.rem(me + o, N_EP)
        push(rout.at[lax.rem(there + x, 2) * 16 + lax.div(there, 2)], rin.at[me],
             bsend.at[o], brecv.at[o], at_ep(there))
    rin[me] = rout[lax.div(me, 2)]

    mixed += project(3) + project(5) + project(4)
    mixed_ref[...] = mixed.astype(BF16)

    for o in RETURN_ORDER:
        await_in(rin.at[lax.rem(me + N_EP - o, N_EP)], bsend.at[o], brecv.at[o])
    returned = rin[...].reshape(N_EP * RBLK, DK)
    moe_ref[...] = (mm(qh_v[...], returned) + mm(ql_v[...], returned)).astype(BF16)

    for copy in pending:
        copy.wait_send()
    for k in range(2):
        for o in SEND_ORDER:
            if o:
                dispatch(k, o).wait_send()
            else:
                @pl.when(c == 1)
                def _():
                    dispatch(k, 0).wait_send()
    for dz in range(1, NZ):
        @pl.when(z + dz < NZ)
        def _():
            along_z(dz).wait_send()


def body(
    mix_query, forget_input, mix_value, out_gate_input, decay_shift, forget_floor, head_gain,
    w_mix_out, moe_input, moe_gain, routes, route_weight, w_exp_gate, w_exp_up, w_exp_down,
):
    vmem = pl.BlockSpec(memory_space=pltpu.VMEM)
    hbm = pl.BlockSpec(memory_space=pl.ANY)
    sem = pltpu.SemaphoreType.DMA
    outs = jax.ShapeDtypeStruct((ROWS, DK), BF16)
    return pl.pallas_call(
        kernel,
        out_shape=(outs, outs),
        in_specs=[hbm] * 4 + [vmem] * 3 + [hbm] * 2 + [vmem] * 3 + [hbm] * 3,
        out_specs=(vmem, vmem),
        scratch_shapes=[
            pltpu.VMEM((4, ROWS, DK), BF16),
            pltpu.VMEM((ROWS, D), BF16),
            pltpu.VMEM((2, ROWS, FPD), BF16),
            pltpu.VMEM((D, FPD), BF16),
            pltpu.VMEM((D, FPD), BF16),
            pltpu.VMEM((NY, FPD, FPD), BF16),
            pltpu.VMEM((D, DK), BF16),
            pltpu.VMEM((2, ROWS, FPD), BF16),
            pltpu.VMEM((2, 16, DBLK, DK), BF16),
            pltpu.VMEM((2, 16, DBLK, DK), BF16),
            pltpu.VMEM((NY, 2, 2, HALF // 2, FPD), BF16),
            pltpu.VMEM((SLOTS, FPD), F32),
            pltpu.VMEM((SLOTS, FPD), F32),
            pltpu.VMEM((SLOTS, FPD), BF16),
            pltpu.VMEM((NY, SLOTS, DK), BF16),
            pltpu.VMEM((NY, SLOTS, DK), BF16),
            pltpu.VMEM((NY, SLOTS, DK), BF16),
            pltpu.VMEM((2, 4, 2, HALF, DK), BF16),
            pltpu.VMEM((2, 4, 2, HALF, DK), BF16),
            pltpu.VMEM((N_EP, RBLK, DK), BF16),
            pltpu.VMEM((N_EP, RBLK, DK), BF16),
            pltpu.VMEM((ROWS, N_EP * RBLK), BF16),
            pltpu.VMEM((ROWS, N_EP * RBLK), BF16),
            pltpu.VMEM((NX, PACK, DK), BF16),
            pltpu.VMEM((NZ, PACK, DK), BF16),
            pltpu.VMEM((2, ROWS, DK), F32),
            pltpu.VMEM((NY, 2, 2, ROWS // 2, DK), BF16),
            sem((12,)), sem((19,)), sem((32,)), sem((32,)), sem((16,)), sem((16,)),
            sem((16,)), sem((16,)), sem((8,)), sem((8,)), sem((16,)), sem((16,)),
            sem((N_EP,)), sem((N_EP,)), sem((NX,)), sem((NX,)), sem((NZ,)), sem((NZ,)),
            sem((16,)), sem((16,)), sem((16,)), sem((16,)),
        ],
        compiler_params=pltpu.CompilerParams(collective_id=0, has_side_effects=True),
        name="step",
    )(
        mix_query, forget_input, mix_value, out_gate_input,
        decay_shift.reshape(1, ROWS), forget_floor.reshape(1, DK), head_gain.reshape(1, DK),
        w_mix_out, moe_input, moe_gain.reshape(1, D), routes.T, route_weight.T,
        w_exp_gate[0], w_exp_up[0], w_exp_down[0],
    )


def solution(mesh):
    torus = Mesh(mesh.devices.reshape(NZ, NX, NY, 2), ("ep_0", "ep_1", "tp_0", "tp_1"))
    placed = (
        P(EP, TP), P(EP, TP), P(EP, TP), P(EP, TP), P(EP, TP), P(TP), P(), P(None, TP),
        P(EP, None), P(), P(EP, None), P(EP, None), P(EP, None, TP), P(EP, None, TP),
        P(EP, TP, None),
    )
    return jax.shard_map(
        body, mesh=torus, in_specs=placed, out_specs=(P(EP, TP), P(EP, TP)), check_vma=False
    )
```

```python
import jax
import jax.numpy as jnp
from jax import lax
from jax.experimental import pallas as pl
from jax.experimental.pallas import tpu as pltpu
from jax.sharding import Mesh
from jax.sharding import PartitionSpec as P

EP = ("ep_0", "ep_1")
TP = ("tp_0", "tp_1")
NZ, NX, NY = 8, 4, 8
N_EP = NZ * NX
ROWS = 256
CAP = 20
D = 2048
DK = 128
FPD = 256
HALF = CAP * N_EP // 2
SLOTS = CAP * N_EP
DBLK = 40
RBLK = 24
SUB = 64
PACK = DK + 16
EPS = 1e-6
MESH = pl.DeviceIdType.MESH
F32 = jnp.float32
BF16 = jnp.bfloat16
I32 = jnp.int32
HIGH = lax.Precision.HIGHEST

SEND_ORDER = (8, 7, 9, 6, 10, 5, 11, 4, 12, 3, 13, 2, 14, 1, 15, 0)
BACK_ORDER = (8, 9, 7, 10, 6, 11, 5, 12, 4, 13, 3, 14, 2, 15, 1, 0)
RETURN_ORDER = sorted(range(1, N_EP), key=lambda o: -min(o, N_EP - o))


def ones_where(mask):
    return jnp.where(mask, 1.0, 0.0).astype(BF16)


def nt_dot(a, b, precision=None):
    return lax.dot_general(
        a, b, (((1,), (1,)), ((), ())), precision=precision, preferred_element_type=F32
    )


def mm(a, b, precision=None):
    return jnp.dot(a, b, precision=precision, preferred_element_type=F32)


def iota(shape, dim):
    return lax.broadcasted_iota(I32, shape, dim)


def kernel(
    q_hbm, f_hbm, v_hbm, og_hbm, shift_hbm, floor_hbm, hgain_hbm, wmix_hbm,
    moe_hbm, gain_hbm, routes_hbm, rw_hbm, wg_hbm, wu_hbm, wd_hbm,
    mixed_ref, moe_ref,
    shift_ref, floor_ref, hgain_ref, gain_ref, routes_ref, rw_ref,
    mixer_v, moe_v, mine_v, wg_v, wu_v, wd_v, wmix_v, norm_v,
    sbuf, rbuf, xs, accg, accu, hid, part, pout, pin, rsend, rrecv,
    rout, rin, qh_v, ql_v, sx, sz, qd_v, hs,
    lsem, wsem, dsend, drecv, asend, arecv, psend, precv, csend, crecv,
    ssend, srecv, bsend, brecv, xsend, xrecv, zsend, zrecv, hsend, hrecv,
    gsend, grecv,
):
    z = lax.axis_index("ep_0")
    x = lax.axis_index("ep_1")
    y = lax.axis_index("tp_0")
    c = lax.axis_index("tp_1")
    me = z * NX + x

    def at_ep(e):
        return (lax.div(e, NX), lax.rem(e, NX), y, c)

    up = (z, x, lax.rem(y + 1, NY), c)
    down = (z, x, lax.rem(y + NY - 1, NY), c)
    partner = (z, x, y, 1 - c)

    def remote(src, dst, send, recv, device):
        return pltpu.make_async_remote_copy(
            src_ref=src, dst_ref=dst, send_sem=send, recv_sem=recv,
            device_id=device, device_id_type=MESH,
        )

    pending = []

    def push(src, dst, send, recv, device):
        copy = remote(src, dst, send, recv, device)
        copy.start()
        pending.append(copy)

    def await_in(dst, send, recv):
        remote(dst, dst, send, recv, partner).wait_recv()

    first_in = [
        pltpu.make_async_copy(routes_hbm, routes_ref, lsem.at[12]),
        pltpu.make_async_copy(gain_hbm, gain_ref, lsem.at[13])]
    for copy in first_in:
        copy.start()
    rows_in = []
    for i in range(4):
        rows_in.append(pltpu.make_async_copy(
            moe_hbm.at[pl.ds(64 * i, 64), :], moe_v.at[pl.ds(64 * i, 64), :], lsem.at[i]))
    rows_in.append(pltpu.make_async_copy(
        moe_hbm.at[:, pl.ds(pl.multiple_of(y * FPD, FPD), FPD)], mine_v.at[0], lsem.at[4]))
    rows_in.append(pltpu.make_async_copy(
        moe_hbm.at[:, pl.ds(pl.multiple_of(lax.rem(y + NY // 2, NY) * FPD, FPD), FPD)],
        mine_v.at[1], lsem.at[6]))
    for copy in rows_in:
        copy.start()
    mixer_in = [
        pltpu.make_async_copy(ref, mixer_v.at[i], lsem.at[7 + i])
        for i, ref in enumerate((f_hbm, v_hbm, q_hbm, og_hbm))]
    mixer_in += [
        pltpu.make_async_copy(a, b, lsem.at[14 + i])
        for i, (a, b) in enumerate((
            (shift_hbm, shift_ref), (floor_hbm, floor_ref), (hgain_hbm, hgain_ref),
            (rw_hbm, rw_ref)))]
    for copy in mixer_in:
        copy.start()

    barrier = pltpu.get_barrier_semaphore()

    def greet(o, carry):
        pl.semaphore_signal(
            barrier, inc=1, device_id=at_ep(lax.rem(me + o, N_EP)), device_id_type=MESH)
        return carry

    lax.fori_loop(1, N_EP, greet, 0)
    for device in (up, down, partner):
        pl.semaphore_signal(barrier, inc=1, device_id=device, device_id_type=MESH)

    weights_in = [
        pltpu.make_async_copy(wg_hbm, wg_v, wsem.at[0]),
        pltpu.make_async_copy(wu_hbm, wu_v, wsem.at[1]),
        pltpu.make_async_copy(wmix_hbm, wmix_v, wsem.at[2]),
    ]
    for i in range(NY):
        for h in range(2):
            column = pl.multiple_of(i * FPD + lax.rem(c + h, 2) * DK, DK)
            weights_in.append(pltpu.make_async_copy(
                wd_hbm.at[:, pl.ds(column, DK)],
                wd_v.at[i, :, pl.ds(h * DK, DK)], wsem.at[3 + 2 * i + h]))
    for copy in weights_in:
        copy.start()

    first_in[0].wait()
    e0, e1 = routes_ref[0:1, :], routes_ref[1:2, :]
    ids = iota((N_EP, ROWS), 0)
    one0, one1 = ids == e0, ids == e1
    ones = jnp.concatenate([ones_where(one0), ones_where(one1)], axis=0)
    strict = ones_where(iota((ROWS, ROWS), 0) < iota((ROWS, ROWS), 1))
    earlier = mm(ones, strict)
    total0 = jnp.sum(jnp.where(one0, 1.0, 0.0), axis=1, keepdims=True)
    rank0 = jnp.sum(jnp.where(one0, earlier[:N_EP], 0.0), axis=0, keepdims=True).astype(I32)
    rank1 = jnp.sum(
        jnp.where(one1, earlier[N_EP:] + total0, 0.0), axis=0, keepdims=True).astype(I32)

    for i in range(4):
        rows_in[i].wait()
    rows_in[4].wait()
    rows_in[5].wait()
    first_in[1].wait()
    halves = (y, lax.rem(y + NY // 2, NY))
    gains = [gain_ref[:, pl.ds(pl.multiple_of(k * FPD, FPD), FPD)] for k in halves]
    for i in range(4):
        block = moe_v[64 * i:64 * i + 64, :].astype(F32)
        mean = jnp.sum(block * block, axis=1, keepdims=True) * (1.0 / D)
        for k in range(2):
            own = mine_v[k, 64 * i:64 * i + 64, :].astype(F32)
            norm_v[k, 64 * i:64 * i + 64, :] = (
                own * lax.rsqrt(mean + EPS) * gains[k]).astype(BF16)

    parity = lax.rem(x + c, 2)
    target0 = jnp.where((e0 & 1) == parity, (e0 >> 1) * DBLK + rank0, -1000)
    target1 = jnp.where((e1 & 1) == parity, (e1 >> 1) * DBLK + rank1, -1000)
    n0 = jnp.concatenate([norm_v[0, :, :DK], norm_v[1, :, :DK]], axis=1)
    n1 = jnp.concatenate([norm_v[0, :, DK:], norm_v[1, :, DK:]], axis=1)
    for g in range(4):
        spot = iota((4 * DBLK, ROWS), 0) + 4 * DBLK * g
        first = ones_where((spot == target0) | (spot == target1))
        second = ones_where((spot == target0 + CAP) | (spot == target1 + CAP))
        rows = (mm(first, n0) + mm(second, n1)).astype(BF16)
        for k in range(2):
            sbuf[k, 4 * g:4 * g + 4] = rows[:, k * DK:(k + 1) * DK].reshape(4, DBLK, DK)

    pl.semaphore_wait(barrier, N_EP + 2)

    def dispatch(k, o):
        expert = lax.rem(me + 2 * o + c, N_EP)
        return remote(sbuf.at[k, lax.div(expert, 2)], rbuf.at[k, lax.div(me, 2)],
                      dsend.at[16 * k + o], drecv.at[16 * k + o], at_ep(expert))

    own_copies = [pltpu.make_async_copy(
        sbuf.at[k, lax.div(me, 2)], rbuf.at[k, lax.div(me, 2)], lsem.at[k * 6 + 5])
        for k in range(2)]
    for k in range(2):
        for o in SEND_ORDER:
            if o:
                dispatch(k, o).start()
            else:
                @pl.when(c == 1)
                def _():
                    dispatch(k, 0).start()

                @pl.when(c == 0)
                def _():
                    own_copies[k].start()

    for copy in mixer_in:
        copy.wait()
    floor = floor_ref[...]
    pre = mixer_v[0].astype(F32)
    forget = floor + (1.0 - floor) * jax.nn.sigmoid(pre)
    keys = (1.0 - floor) * jax.nn.sigmoid(-pre)
    shift = jnp.transpose(jnp.broadcast_to(shift_ref[...], (DK, ROWS)))
    log_decay = jnp.log(forget) + shift
    lower = jnp.where(iota((ROWS, ROWS), 0) >= iota((ROWS, ROWS), 1), 1.0, 0.0)
    running = mm(lower, log_decay, HIGH)
    values = mixer_v[1].astype(F32)
    query = mixer_v[2].astype(F32)
    closing = running[ROWS - 1:ROWS, :]
    values_t = jnp.transpose(values)
    state_t = mm(values_t, keys * jnp.exp(closing - running), HIGH)
    sx[x, 0:DK, :] = state_t.astype(BF16)
    sx[x, DK:PACK, :] = jnp.broadcast_to(jnp.exp(closing), (PACK - DK, DK)).astype(BF16)
    for dx in range(1, NX):
        push(sx.at[x], sx.at[x], xsend.at[dx], xrecv.at[dx],
             (z, lax.rem(x + dx, NX), y, c))

    def arrived(k):
        for o in SEND_ORDER:
            source = lax.rem(me + N_EP - 2 * o + N_EP - c, N_EP)
            slot = rbuf.at[k, lax.div(source, 2)]
            if o:
                await_in(slot, dsend.at[16 * k + o], drecv.at[16 * k + o])
            else:
                @pl.when(c == 1)
                def _():
                    await_in(slot, dsend.at[16 * k], drecv.at[16 * k])

                @pl.when(c == 0)
                def _():
                    own_copies[k].wait()

    row, col = iota((4 * CAP, 4 * DBLK), 0), iota((4 * CAP, 4 * DBLK), 1)
    spot = row + (DBLK - CAP) * ((row * 3277) >> 16)
    packs = [ones_where(col == spot + CAP * h) for h in range(2)]

    def pack(k):
        arrived(k)
        for g in range(4):
            block = rbuf[k, 4 * g:4 * g + 4].reshape(4 * DBLK, DK)
            for h in range(2):
                xs[halves[k], c, g // 2, (g % 2) * 80:(g % 2) * 80 + 80,
                   h * DK:(h + 1) * DK] = mm(packs[h], block).astype(BF16)

    pack(0)

    def slab(j):
        return lax.rem(y + j, NY)

    def ring_send(buf, direction, hop, sub, send, recv):
        j = (NY - hop) % NY if direction == 0 else hop
        index = direction * 8 + hop * 2 + sub
        push(buf.at[slab(j), c, sub], buf.at[slab(j), c, sub], send.at[index], recv.at[index],
             up if direction == 0 else down)

    def ring_take(buf, direction, hop, sub, send, recv):
        j = (NY - hop) % NY if direction == 0 else hop
        index = direction * 8 + (hop - 1) * 2 + sub
        await_in(buf.at[slab(j), c, sub], send.at[index], recv.at[index])
        return j

    def pair_send(buf, j, sub, send, recv):
        push(buf.at[slab(j), c, sub], buf.at[slab(j), c, sub],
             send.at[2 * j + sub], recv.at[2 * j + sub], partner)

    def pair_take(buf, j, sub, send, recv):
        await_in(buf.at[slab(j), 1 - c, sub], send.at[2 * j + sub], recv.at[2 * j + sub])

    far, near = ((0, 0), (1, 1)), ((0, 1), (1, 0))

    def gather_start(buf, send, recv, psend, precv):
        for direction, sub in far + near:
            ring_send(buf, direction, 0, sub, send, recv)
        for sub in range(2):
            pair_send(buf, 0, sub, psend, precv)

    def gather_hop(buf, hop, send, recv, psend, precv):
        for direction, sub in far + (near if hop < 4 else ()):
            j = ring_take(buf, direction, hop, sub, send, recv)
            if hop < (4 if (direction, sub) in far else 3):
                ring_send(buf, direction, hop, sub, send, recv)
            pair_send(buf, j, sub, psend, precv)

    for sub in range(2):
        for direction in range(2):
            ring_send(xs, direction, 0, sub, asend, arecv)
        pair_send(xs, 0, sub, psend, precv)

    def rows_hop(hop, sub):
        for direction in range(2):
            j = ring_take(xs, direction, hop, sub, asend, arecv)
            if hop < 3:
                ring_send(xs, direction, hop, sub, asend, arecv)
            pair_send(xs, j, sub, psend, precv)


    def read_state(ref, k):
        return ref[k, DK:PACK, :].astype(F32)[0:1], ref[k, 0:DK, :].astype(F32)

    def step(before, after):
        return before[0] * after[0], after[0] * before[1] + after[1]

    def prefix(ref, count, index):
        running = (jnp.ones((1, DK), F32), jnp.zeros((DK, DK), F32))
        inside = running
        for k in range(count):
            running = step(running, read_state(ref, k))
            inside = tuple(jnp.where(k < index, a, b) for a, b in zip(running, inside))
        return inside, running

    for dx in range(1, NX):
        await_in(sx.at[lax.rem(x + NX - dx, NX)], xsend.at[dx], xrecv.at[dx])
    inside_x, whole = prefix(sx, NX, x)
    sz[z, 0:DK, :] = whole[1].astype(BF16)
    sz[z, DK:PACK, :] = jnp.broadcast_to(whole[0], (PACK - DK, DK)).astype(BF16)

    def along_z(dz):
        return remote(sz.at[z], sz.at[z], zsend.at[dz], zrecv.at[dz],
                      (lax.rem(z + dz, NZ), x, y, c))

    for dz in range(1, NZ):
        @pl.when(z + dz < NZ)
        def _():
            along_z(dz).start()

    causal = iota((SUB, SUB), 0) >= iota((SUB, SUB), 1)
    local = []
    for i in range(ROWS // SUB):
        lo, hi = i * SUB, (i + 1) * SUB
        decay_i, query_i = running[lo:hi], query[lo:hi]
        middle = running[lo + SUB // 2 - 1:lo + SUB // 2]
        scores = jnp.where(causal, nt_dot(
            query_i * jnp.exp(decay_i - middle), keys[lo:hi] * jnp.exp(middle - decay_i),
            HIGH), 0.0)
        out = mm(scores, values[lo:hi], HIGH)
        if i:
            start = running[lo - 1:lo]
            scores = nt_dot(query_i * jnp.exp(decay_i - start),
                            keys[:lo] * jnp.exp(start - running[:lo]), HIGH)
            out = out + mm(scores, values[:lo], HIGH)
        local.append(out)
    qd_v[0] = jnp.concatenate(local, axis=0)
    qd_v[1] = query * jnp.exp(running)


    weights_in[0].wait()
    weights_in[1].wait()

    def expert_in(half, *slabs):
        for j in slabs:
            pair_take(xs, j, half, psend, precv)
            rows = jnp.concatenate([xs[slab(j), 0, half], xs[slab(j), 1, half]], axis=0)
            depth = pl.ds(pl.multiple_of(slab(j) * FPD, FPD), FPD)
            gate, raised = mm(rows, wg_v[depth, :]), mm(rows, wu_v[depth, :])
            if j == 0:
                accg[half], accu[half] = gate, raised
            else:
                accg[half] += gate
                accu[half] += raised

    def expert_hidden(half):
        for i in range(2):
            block = slice(160 * i, 160 * i + 160)
            hid[half, block, :] = (
                jax.nn.silu(accg[half, block, :]) * accu[half, block, :]).astype(BF16)

    def expert_out(half, *slabs):
        for j in slabs:
            partial = mm(hid[half], wd_v[slab(j)]).astype(BF16)
            part[j, half] = partial[:, :DK]
            pout[j, half] = partial[:, DK:]
            push(pout.at[j, half], pin.at[j, half],
                 csend.at[2 * j + half], crecv.at[2 * j + half], partner)

    summed = set()

    def chip_sum(j, half, side):
        if (j, half) not in summed:
            summed.add((j, half))
            await_in(pin.at[j, half], csend.at[2 * j + half], crecv.at[2 * j + half])
        block = slice(160 * side, 160 * side + 160)
        return part[j, half, block, :].astype(F32) + pin[j, half, block, :].astype(F32)

    def sum_index(direction, step, side, half):
        return (direction * 8 + step * 2 + side) * 2 + half

    def sum_send(direction, step, side, half, value):
        index = sum_index(direction, step, side, half)
        rsend[direction, step, side, half] = value.astype(BF16)
        push(rsend.at[direction, step, side, half], rrecv.at[direction, step, side, half],
             ssend.at[index], srecv.at[index], up if direction == 0 else down)

    def sum_take(direction, step, side, half):
        index = sum_index(direction, step, side, half)
        await_in(rrecv.at[direction, step, side, half], ssend.at[index], srecv.at[index])
        return rrecv[direction, step, side, half].astype(F32)

    def target(direction, side, step):
        j = (4 if (direction, side) in far else 3) - step
        return j % NY if direction == 0 else -j % NY

    def sum_start(half, parts):
        for direction, side in parts:
            sum_send(direction, 0, side, half,
                     chip_sum(target(direction, side, 0), half, side))

    def sum_hop(step, half, parts):
        for direction, side in parts:
            value = sum_take(direction, step - 1, side, half)
            sum_send(direction, step, side, half,
                     value + chip_sum(target(direction, side, step), half, side))

    rows_hop(1, 0)
    rows_hop(1, 1)
    expert_in(0, 0)
    expert_in(1, 0)
    rows_hop(2, 0)
    expert_in(0, 1, 7)
    rows_hop(2, 1)
    pack(1)
    for sub in range(2):
        pair_send(xs, 4, sub, psend, precv)

    for dz in range(1, NZ):
        @pl.when(z >= dz)
        def _():
            await_in(sz.at[lax.rem(z + NZ - dz, NZ)], zsend.at[dz], zrecv.at[dz])

    before, _ = prefix(sz, NZ, z)
    incoming = step(before, inside_x)[1]
    result = qd_v[0] + nt_dot(qd_v[1], incoming, HIGH)
    inverse = lax.rsqrt(jnp.mean(result * result, axis=1, keepdims=True) + EPS)
    head_out = result * inverse * hgain_ref[...] * jax.nn.silu(mixer_v[3].astype(F32))
    hs[y, c] = head_out.astype(BF16).reshape(2, ROWS // 2, DK)

    gather_start(hs, hsend, hrecv, gsend, grecv)
    expert_in(1, 1, 7)
    for copy in weights_in[2:]:
        copy.wait()

    slot0 = (e0 * RBLK + rank0).astype(F32)
    slot1 = (e1 * RBLK + rank1).astype(F32)
    which = iota((DK, ROWS), 0)
    table = jnp.where(which == 0, slot0, jnp.where(which == 1, slot1, jnp.where(
        which == 2, rw_ref[0:1, :], jnp.where(which == 3, rw_ref[1:2, :], 0.0))))
    table = jnp.transpose(table)
    place0, place1 = table[:, 0:1].astype(I32), table[:, 1:2].astype(I32)
    for g in range(N_EP * RBLK // 256):
        spot = iota((ROWS, 256), 1) + 256 * g
        weight = jnp.where(spot == place0, table[:, 2:3], 0.0) + jnp.where(
            spot == place1, table[:, 3:4], 0.0)
        high = weight.astype(BF16)
        qh_v[:, 256 * g:256 * g + 256] = high
        ql_v[:, 256 * g:256 * g + 256] = (weight - high.astype(F32)).astype(BF16)

    rows_hop(3, 0)
    expert_in(0, 2, 6, 4)
    expert_in(1, 2, 6)
    expert_in(0, 3, 5)
    expert_hidden(0)
    expert_out(0, 4)
    rows_hop(3, 1)
    expert_out(0, 3, 5)
    expert_in(1, 4)
    sum_start(0, far)
    expert_in(1, 3, 5)
    sum_start(0, near)
    expert_hidden(1)
    expert_out(1, 4, 3, 5)
    gather_hop(hs, 1, hsend, hrecv, gsend, grecv)
    expert_out(0, 2, 6)
    sum_start(1, far)
    sum_start(1, near)
    expert_out(1, 2, 6)
    gather_hop(hs, 2, hsend, hrecv, gsend, grecv)

    def project(j):
        for sub in range(2):
            pair_take(hs, j, sub, gsend, grecv)
        heads = hs[slab(j)].reshape(2, ROWS, DK)
        rows = jnp.concatenate([heads[0], heads[1]], axis=1)
        return mm(rows, wmix_v[pl.ds(pl.multiple_of(slab(j) * FPD, FPD), FPD), :])

    row, col = iota((4 * RBLK, 4 * CAP), 0), iota((4 * RBLK, 4 * CAP), 1)
    group = (row * 2731) >> 16
    spread = ones_where((col == row - (RBLK - CAP) * group) & (row - RBLK * group < CAP))

    def give_back(o, half):
        there = 16 * half + lax.rem(me + o, 16)
        return remote(rout.at[lax.rem(there + x, 2) * 16 + lax.div(there, 2)], rin.at[me],
                      bsend.at[16 * half + o], brecv.at[me], at_ep(there))

    def finish(half):
        for side in range(2):
            value = chip_sum(0, half, side)
            for direction in range(2):
                value = value + sum_take(direction, 3 if (direction, side) in far else 2,
                                         side, half)
            for g in range(2):
                place = 16 * side + 8 * half + 4 * g
                rout[place:place + 4] = mm(
                    spread, value[80 * g:80 * g + 80].astype(BF16)
                ).astype(BF16).reshape(4, RBLK, DK)
        for o in BACK_ORDER:
            if o:
                give_back(o, half).start()
            else:
                @pl.when(lax.div(me, 16) != half)
                def _():
                    give_back(0, half).start()

    sum_hop(1, 0, far)
    expert_out(0, 1, 7, 0)
    sum_hop(1, 0, near)
    sum_hop(1, 1, far)
    expert_out(1, 1, 7, 0)
    sum_hop(1, 1, near)
    gather_hop(hs, 3, hsend, hrecv, gsend, grecv)
    mixed = project(0)
    sum_hop(2, 0, far)
    sum_hop(2, 0, near)
    sum_hop(2, 1, far)
    sum_hop(2, 1, near)
    gather_hop(hs, 4, hsend, hrecv, gsend, grecv)
    mixed += project(1) + project(7)
    sum_hop(3, 0, far)
    mixed += project(2) + project(6)
    sum_hop(3, 1, far)
    finish(0)
    finish(1)
    rin[me] = rout[lax.div(me, 2)]
    mixed += project(3) + project(5) + project(4)
    mixed_ref[...] = mixed.astype(BF16)

    for o in RETURN_ORDER:
        there = lax.rem(me + o, N_EP)
        await_in(rin.at[there], bsend.at[o], brecv.at[there])
    returned = rin[...].reshape(N_EP * RBLK, DK)
    moe_ref[...] = (mm(qh_v[...], returned) + mm(ql_v[...], returned)).astype(BF16)

    for copy in pending:
        copy.wait_send()
    for k in range(2):
        for o in SEND_ORDER:
            if o:
                dispatch(k, o).wait_send()
            else:
                @pl.when(c == 1)
                def _():
                    dispatch(k, 0).wait_send()
    for dz in range(1, NZ):
        @pl.when(z + dz < NZ)
        def _():
            along_z(dz).wait_send()

    for half in range(2):
        for o in BACK_ORDER:
            if o:
                give_back(o, half).wait_send()
            else:
                @pl.when(lax.div(me, 16) != half)
                def _():
                    give_back(0, half).wait_send()

def body(
    mix_query, forget_input, mix_value, out_gate_input, decay_shift, forget_floor, head_gain,
    w_mix_out, moe_input, moe_gain, routes, route_weight, w_exp_gate, w_exp_up, w_exp_down,
):
    vmem = pl.BlockSpec(memory_space=pltpu.VMEM)
    hbm = pl.BlockSpec(memory_space=pl.ANY)
    sem = pltpu.SemaphoreType.DMA
    outs = jax.ShapeDtypeStruct((ROWS, DK), BF16)
    return pl.pallas_call(
        kernel,
        out_shape=(outs, outs),
        in_specs=[hbm] * 15,
        out_specs=(vmem, vmem),
        scratch_shapes=[
            pltpu.VMEM((1, ROWS), F32),
            pltpu.VMEM((1, DK), F32),
            pltpu.VMEM((1, DK), F32),
            pltpu.VMEM((1, D), F32),
            pltpu.VMEM((2, ROWS), I32),
            pltpu.VMEM((2, ROWS), F32),
            pltpu.VMEM((4, ROWS, DK), BF16),
            pltpu.VMEM((ROWS, D), BF16),
            pltpu.VMEM((2, ROWS, FPD), BF16),
            pltpu.VMEM((D, FPD), BF16),
            pltpu.VMEM((D, FPD), BF16),
            pltpu.VMEM((NY, FPD, FPD), BF16),
            pltpu.VMEM((D, DK), BF16),
            pltpu.VMEM((2, ROWS, FPD), BF16),
            pltpu.VMEM((2, 16, DBLK, DK), BF16),
            pltpu.VMEM((2, 16, DBLK, DK), BF16),
            pltpu.VMEM((NY, 2, 2, HALF // 2, FPD), BF16),
            pltpu.VMEM((2, HALF, FPD), F32),
            pltpu.VMEM((2, HALF, FPD), F32),
            pltpu.VMEM((2, HALF, FPD), BF16),
            pltpu.VMEM((NY, 2, HALF, DK), BF16),
            pltpu.VMEM((NY, 2, HALF, DK), BF16),
            pltpu.VMEM((NY, 2, HALF, DK), BF16),
            pltpu.VMEM((2, 4, 2, 2, HALF // 2, DK), BF16),
            pltpu.VMEM((2, 4, 2, 2, HALF // 2, DK), BF16),
            pltpu.VMEM((N_EP, RBLK, DK), BF16),
            pltpu.VMEM((N_EP, RBLK, DK), BF16),
            pltpu.VMEM((ROWS, N_EP * RBLK), BF16),
            pltpu.VMEM((ROWS, N_EP * RBLK), BF16),
            pltpu.VMEM((NX, PACK, DK), BF16),
            pltpu.VMEM((NZ, PACK, DK), BF16),
            pltpu.VMEM((2, ROWS, DK), F32),
            pltpu.VMEM((NY, 2, 2, ROWS // 2, DK), BF16),
            sem((18,)), sem((19,)), sem((32,)), sem((32,)), sem((16,)), sem((16,)),
            sem((16,)), sem((16,)), sem((16,)), sem((16,)), sem((32,)), sem((32,)),
            sem((N_EP,)), sem((N_EP,)), sem((NX,)), sem((NX,)), sem((NZ,)), sem((NZ,)),
            sem((16,)), sem((16,)), sem((16,)), sem((16,)),
        ],
        compiler_params=pltpu.CompilerParams(collective_id=0, has_side_effects=True),
        name="step",
    )(
        mix_query, forget_input, mix_value, out_gate_input,
        decay_shift.reshape(1, ROWS), forget_floor.reshape(1, DK), head_gain.reshape(1, DK),
        w_mix_out, moe_input, moe_gain.reshape(1, D), routes.T, route_weight.T,
        w_exp_gate[0], w_exp_up[0], w_exp_down[0],
    )


def solution(mesh):
    torus = Mesh(mesh.devices.reshape(NZ, NX, NY, 2), ("ep_0", "ep_1", "tp_0", "tp_1"))
    placed = (
        P(EP, TP), P(EP, TP), P(EP, TP), P(EP, TP), P(EP, TP), P(TP), P(), P(None, TP),
        P(EP, None), P(), P(EP, None), P(EP, None), P(EP, None, TP), P(EP, None, TP),
        P(EP, TP, None),
    )
    return jax.shard_map(
        body, mesh=torus, in_specs=placed, out_specs=(P(EP, TP), P(EP, TP)), check_vma=False
    )
```

```python
import jax
import jax.numpy as jnp
from jax import lax
from jax.experimental import pallas as pl
from jax.experimental.pallas import tpu as pltpu
from jax.sharding import Mesh
from jax.sharding import PartitionSpec as P

EP = ("ep_0", "ep_1")
TP = ("tp_0", "tp_1")
NZ, NX, NY = 8, 4, 8
N_EP = NZ * NX
ROWS = 256
CAP = 20
D = 2048
DK = 128
FPD = 256
HALF = CAP * N_EP // 2
SLOTS = CAP * N_EP
DBLK = 40
RBLK = 24
SUB = 64
PACK = DK + 16
EPS = 1e-6
MESH = pl.DeviceIdType.MESH
F32 = jnp.float32
BF16 = jnp.bfloat16
I32 = jnp.int32
HIGH = lax.Precision.HIGHEST

SEND_ORDER = (8, 7, 9, 6, 10, 5, 11, 4, 12, 3, 13, 2, 14, 1, 15, 0)
BACK_ORDER = (8, 9, 7, 10, 6, 11, 5, 12, 4, 13, 3, 14, 2, 15, 1, 0)
RETURN_ORDER = sorted(range(1, N_EP), key=lambda o: -min(o, N_EP - o))


def ones_where(mask):
    return jnp.where(mask, 1.0, 0.0).astype(BF16)


def nt_dot(a, b, precision=None):
    return lax.dot_general(
        a, b, (((1,), (1,)), ((), ())), precision=precision, preferred_element_type=F32
    )


def mm(a, b, precision=None):
    return jnp.dot(a, b, precision=precision, preferred_element_type=F32)


def iota(shape, dim):
    return lax.broadcasted_iota(I32, shape, dim)


def kernel(
    q_hbm, f_hbm, v_hbm, og_hbm, shift_hbm, floor_hbm, hgain_hbm, wmix_hbm,
    moe_hbm, gain_hbm, routes_hbm, rw_hbm, wg_hbm, wu_hbm, wd_hbm,
    mixed_ref, moe_ref,
    shift_ref, floor_ref, hgain_ref, gain_ref, routes_ref, rw_ref,
    mixer_v, moe_v, mine_v, wg_v, wu_v, wd_v, wmix_v, norm_v,
    sbuf, rbuf, xs, accg, accu, hid, part, pout, pin, rsend, rrecv,
    rout, rin, qh_v, ql_v, sx, sz, qd_v, hs,
    lsem, wsem, dsend, drecv, asend, arecv, psend, precv, csend, crecv,
    ssend, srecv, bsend, brecv, xsend, xrecv, zsend, zrecv, hsend, hrecv,
    gsend, grecv,
):
    z = lax.axis_index("ep_0")
    x = lax.axis_index("ep_1")
    y = lax.axis_index("tp_0")
    c = lax.axis_index("tp_1")
    me = z * NX + x

    def at_ep(e):
        return (lax.div(e, NX), lax.rem(e, NX), y, c)

    up = (z, x, lax.rem(y + 1, NY), c)
    down = (z, x, lax.rem(y + NY - 1, NY), c)
    partner = (z, x, y, 1 - c)

    def remote(src, dst, send, recv, device):
        return pltpu.make_async_remote_copy(
            src_ref=src, dst_ref=dst, send_sem=send, recv_sem=recv,
            device_id=device, device_id_type=MESH,
        )

    pending = []

    def push(src, dst, send, recv, device):
        copy = remote(src, dst, send, recv, device)
        copy.start()
        pending.append(copy)

    def await_in(dst, send, recv):
        remote(dst, dst, send, recv, partner).wait_recv()

    first_in = [
        pltpu.make_async_copy(routes_hbm, routes_ref, lsem.at[12]),
        pltpu.make_async_copy(gain_hbm, gain_ref, lsem.at[13])]
    for copy in first_in:
        copy.start()
    rows_in = []
    for i in range(4):
        rows_in.append(pltpu.make_async_copy(
            moe_hbm.at[pl.ds(64 * i, 64), :], moe_v.at[pl.ds(64 * i, 64), :], lsem.at[i]))
    rows_in.append(pltpu.make_async_copy(
        moe_hbm.at[:, pl.ds(pl.multiple_of(y * FPD, FPD), FPD)], mine_v.at[0], lsem.at[4]))
    rows_in.append(pltpu.make_async_copy(
        moe_hbm.at[:, pl.ds(pl.multiple_of(lax.rem(y + NY // 2, NY) * FPD, FPD), FPD)],
        mine_v.at[1], lsem.at[6]))
    for copy in rows_in:
        copy.start()
    mixer_in = [
        pltpu.make_async_copy(ref, mixer_v.at[i], lsem.at[7 + i])
        for i, ref in enumerate((f_hbm, v_hbm, q_hbm, og_hbm))]
    mixer_in += [
        pltpu.make_async_copy(a, b, lsem.at[14 + i])
        for i, (a, b) in enumerate((
            (shift_hbm, shift_ref), (floor_hbm, floor_ref), (hgain_hbm, hgain_ref),
            (rw_hbm, rw_ref)))]
    for copy in mixer_in:
        copy.start()

    barrier = pltpu.get_barrier_semaphore()

    def greet(o, carry):
        pl.semaphore_signal(
            barrier, inc=1, device_id=at_ep(lax.rem(me + o, N_EP)), device_id_type=MESH)
        return carry

    lax.fori_loop(1, N_EP, greet, 0)
    for device in (up, down, partner):
        pl.semaphore_signal(barrier, inc=1, device_id=device, device_id_type=MESH)

    weights_in = [
        pltpu.make_async_copy(wg_hbm, wg_v, wsem.at[0]),
        pltpu.make_async_copy(wu_hbm, wu_v, wsem.at[1]),
        pltpu.make_async_copy(wmix_hbm, wmix_v, wsem.at[2]),
    ]
    for i in range(NY):
        for h in range(2):
            column = pl.multiple_of(i * FPD + lax.rem(c + h, 2) * DK, DK)
            weights_in.append(pltpu.make_async_copy(
                wd_hbm.at[:, pl.ds(column, DK)],
                wd_v.at[i, :, pl.ds(h * DK, DK)], wsem.at[3 + 2 * i + h]))
    for copy in weights_in:
        copy.start()

    first_in[0].wait()
    e0, e1 = routes_ref[0:1, :], routes_ref[1:2, :]
    ids = iota((N_EP, ROWS), 0)
    one0, one1 = ids == e0, ids == e1
    ones = jnp.concatenate([ones_where(one0), ones_where(one1)], axis=0)
    strict = ones_where(iota((ROWS, ROWS), 0) < iota((ROWS, ROWS), 1))
    earlier = mm(ones, strict)
    total0 = jnp.sum(jnp.where(one0, 1.0, 0.0), axis=1, keepdims=True)
    rank0 = jnp.sum(jnp.where(one0, earlier[:N_EP], 0.0), axis=0, keepdims=True).astype(I32)
    rank1 = jnp.sum(
        jnp.where(one1, earlier[N_EP:] + total0, 0.0), axis=0, keepdims=True).astype(I32)

    for i in range(4):
        rows_in[i].wait()
    rows_in[4].wait()
    rows_in[5].wait()
    first_in[1].wait()
    halves = (y, lax.rem(y + NY // 2, NY))
    gains = [gain_ref[:, pl.ds(pl.multiple_of(k * FPD, FPD), FPD)] for k in halves]
    for i in range(4):
        block = moe_v[64 * i:64 * i + 64, :].astype(F32)
        mean = jnp.sum(block * block, axis=1, keepdims=True) * (1.0 / D)
        for k in range(2):
            own = mine_v[k, 64 * i:64 * i + 64, :].astype(F32)
            norm_v[k, 64 * i:64 * i + 64, :] = (
                own * lax.rsqrt(mean + EPS) * gains[k]).astype(BF16)

    parity = lax.rem(x + c, 2)
    target0 = jnp.where((e0 & 1) == parity, (e0 >> 1) * DBLK + rank0, -1000)
    target1 = jnp.where((e1 & 1) == parity, (e1 >> 1) * DBLK + rank1, -1000)
    n0 = jnp.concatenate([norm_v[0, :, :DK], norm_v[1, :, :DK]], axis=1)
    n1 = jnp.concatenate([norm_v[0, :, DK:], norm_v[1, :, DK:]], axis=1)
    for g in range(4):
        spot = iota((4 * DBLK, ROWS), 0) + 4 * DBLK * g
        first = ones_where((spot == target0) | (spot == target1))
        second = ones_where((spot == target0 + CAP) | (spot == target1 + CAP))
        rows = (mm(first, n0) + mm(second, n1)).astype(BF16)
        for k in range(2):
            sbuf[k, 4 * g:4 * g + 4] = rows[:, k * DK:(k + 1) * DK].reshape(4, DBLK, DK)

    pl.semaphore_wait(barrier, N_EP + 2)

    def dispatch(k, o):
        expert = lax.rem(me + 2 * o + c, N_EP)
        return remote(sbuf.at[k, lax.div(expert, 2)], rbuf.at[k, lax.div(me, 2)],
                      dsend.at[16 * k + o], drecv.at[16 * k + o], at_ep(expert))

    own_copies = [pltpu.make_async_copy(
        sbuf.at[k, lax.div(me, 2)], rbuf.at[k, lax.div(me, 2)], lsem.at[k * 6 + 5])
        for k in range(2)]
    for k in range(2):
        for o in SEND_ORDER:
            if o:
                dispatch(k, o).start()
            else:
                @pl.when(c == 1)
                def _():
                    dispatch(k, 0).start()

                @pl.when(c == 0)
                def _():
                    own_copies[k].start()

    for copy in mixer_in:
        copy.wait()
    floor = floor_ref[...]
    pre = mixer_v[0].astype(F32)
    forget = floor + (1.0 - floor) * jax.nn.sigmoid(pre)
    keys = (1.0 - floor) * jax.nn.sigmoid(-pre)
    shift = jnp.transpose(jnp.broadcast_to(shift_ref[...], (DK, ROWS)))
    log_decay = jnp.log(forget) + shift
    lower = jnp.where(iota((ROWS, ROWS), 0) >= iota((ROWS, ROWS), 1), 1.0, 0.0)
    running = mm(lower, log_decay, HIGH)
    values = mixer_v[1].astype(F32)
    query = mixer_v[2].astype(F32)
    closing = running[ROWS - 1:ROWS, :]
    values_t = jnp.transpose(values)
    state_t = mm(values_t, keys * jnp.exp(closing - running), HIGH)
    sx[x, 0:DK, :] = state_t.astype(BF16)
    sx[x, DK:PACK, :] = jnp.broadcast_to(jnp.exp(closing), (PACK - DK, DK)).astype(BF16)
    for dx in range(1, NX):
        push(sx.at[x], sx.at[x], xsend.at[dx], xrecv.at[dx],
             (z, lax.rem(x + dx, NX), y, c))

    def arrived(k):
        for o in SEND_ORDER:
            source = lax.rem(me + N_EP - 2 * o + N_EP - c, N_EP)
            slot = rbuf.at[k, lax.div(source, 2)]
            if o:
                await_in(slot, dsend.at[16 * k + o], drecv.at[16 * k + o])
            else:
                @pl.when(c == 1)
                def _():
                    await_in(slot, dsend.at[16 * k], drecv.at[16 * k])

                @pl.when(c == 0)
                def _():
                    own_copies[k].wait()

    row, col = iota((4 * CAP, 4 * DBLK), 0), iota((4 * CAP, 4 * DBLK), 1)
    spot = row + (DBLK - CAP) * ((row * 3277) >> 16)
    packs = [ones_where(col == spot + CAP * h) for h in range(2)]

    def pack(k):
        arrived(k)
        for g in range(4):
            block = rbuf[k, 4 * g:4 * g + 4].reshape(4 * DBLK, DK)
            for h in range(2):
                xs[halves[k], c, g // 2, (g % 2) * 80:(g % 2) * 80 + 80,
                   h * DK:(h + 1) * DK] = mm(packs[h], block).astype(BF16)

    pack(0)

    def slab(j):
        return lax.rem(y + j, NY)

    def ring_send(buf, direction, hop, sub, send, recv):
        j = (NY - hop) % NY if direction == 0 else hop
        index = direction * 8 + hop * 2 + sub
        push(buf.at[slab(j), c, sub], buf.at[slab(j), c, sub], send.at[index], recv.at[index],
             up if direction == 0 else down)

    def ring_take(buf, direction, hop, sub, send, recv):
        j = (NY - hop) % NY if direction == 0 else hop
        index = direction * 8 + (hop - 1) * 2 + sub
        await_in(buf.at[slab(j), c, sub], send.at[index], recv.at[index])
        return j

    def pair_send(buf, j, sub, send, recv):
        push(buf.at[slab(j), c, sub], buf.at[slab(j), c, sub],
             send.at[2 * j + sub], recv.at[2 * j + sub], partner)

    def pair_take(buf, j, sub, send, recv):
        await_in(buf.at[slab(j), 1 - c, sub], send.at[2 * j + sub], recv.at[2 * j + sub])

    far, near = ((0, 0), (1, 1)), ((0, 1), (1, 0))

    def gather_start(buf, send, recv, psend, precv):
        for direction, sub in far + near:
            ring_send(buf, direction, 0, sub, send, recv)
        for sub in range(2):
            pair_send(buf, 0, sub, psend, precv)

    def gather_hop(buf, hop, send, recv, psend, precv):
        for direction, sub in far + (near if hop < 4 else ()):
            j = ring_take(buf, direction, hop, sub, send, recv)
            if hop < (4 if (direction, sub) in far else 3):
                ring_send(buf, direction, hop, sub, send, recv)
            pair_send(buf, j, sub, psend, precv)

    for sub in range(2):
        for direction in range(2):
            ring_send(xs, direction, 0, sub, asend, arecv)
        pair_send(xs, 0, sub, psend, precv)

    def rows_hop(hop, sub):
        for direction in range(2):
            j = ring_take(xs, direction, hop, sub, asend, arecv)
            if hop < 3:
                ring_send(xs, direction, hop, sub, asend, arecv)
            pair_send(xs, j, sub, psend, precv)


    def read_state(ref, k):
        return ref[k, DK:PACK, :].astype(F32)[0:1], ref[k, 0:DK, :].astype(F32)

    def step(before, after):
        return before[0] * after[0], after[0] * before[1] + after[1]

    def prefix(ref, count, index):
        running = (jnp.ones((1, DK), F32), jnp.zeros((DK, DK), F32))
        inside = running
        for k in range(count):
            running = step(running, read_state(ref, k))
            inside = tuple(jnp.where(k < index, a, b) for a, b in zip(running, inside))
        return inside, running

    for dx in range(1, NX):
        await_in(sx.at[lax.rem(x + NX - dx, NX)], xsend.at[dx], xrecv.at[dx])
    inside_x, whole = prefix(sx, NX, x)
    sz[z, 0:DK, :] = whole[1].astype(BF16)
    sz[z, DK:PACK, :] = jnp.broadcast_to(whole[0], (PACK - DK, DK)).astype(BF16)

    def along_z(dz):
        return remote(sz.at[z], sz.at[z], zsend.at[dz], zrecv.at[dz],
                      (lax.rem(z + dz, NZ), x, y, c))

    for dz in range(1, NZ):
        @pl.when(z + dz < NZ)
        def _():
            along_z(dz).start()

    causal = iota((SUB, SUB), 0) >= iota((SUB, SUB), 1)
    local = []
    for i in range(ROWS // SUB):
        lo, hi = i * SUB, (i + 1) * SUB
        decay_i, query_i = running[lo:hi], query[lo:hi]
        middle = running[lo + SUB // 2 - 1:lo + SUB // 2]
        scores = jnp.where(causal, nt_dot(
            query_i * jnp.exp(decay_i - middle), keys[lo:hi] * jnp.exp(middle - decay_i),
            HIGH), 0.0)
        out = mm(scores, values[lo:hi], HIGH)
        if i:
            start = running[lo - 1:lo]
            scores = nt_dot(query_i * jnp.exp(decay_i - start),
                            keys[:lo] * jnp.exp(start - running[:lo]), HIGH)
            out = out + mm(scores, values[:lo], HIGH)
        local.append(out)
    qd_v[0] = jnp.concatenate(local, axis=0)
    qd_v[1] = query * jnp.exp(running)


    weights_in[0].wait()
    weights_in[1].wait()

    def expert_in(half, *slabs):
        for j in slabs:
            pair_take(xs, j, half, psend, precv)
            rows = jnp.concatenate([xs[slab(j), 0, half], xs[slab(j), 1, half]], axis=0)
            depth = pl.ds(pl.multiple_of(slab(j) * FPD, FPD), FPD)
            gate, raised = mm(rows, wg_v[depth, :]), mm(rows, wu_v[depth, :])
            if j == 0:
                accg[half], accu[half] = gate, raised
            else:
                accg[half] += gate
                accu[half] += raised

    def expert_hidden(half):
        for i in range(2):
            block = slice(160 * i, 160 * i + 160)
            hid[half, block, :] = (
                jax.nn.silu(accg[half, block, :]) * accu[half, block, :]).astype(BF16)

    def expert_out(half, *slabs):
        for j in slabs:
            partial = mm(hid[half], wd_v[slab(j)]).astype(BF16)
            part[j, half] = partial[:, :DK]
            pout[j, half] = partial[:, DK:]
            push(pout.at[j, half], pin.at[j, half],
                 csend.at[2 * j + half], crecv.at[2 * j + half], partner)

    summed = set()

    def chip_sum(j, half, side):
        if (j, half) not in summed:
            summed.add((j, half))
            await_in(pin.at[j, half], csend.at[2 * j + half], crecv.at[2 * j + half])
        block = slice(160 * side, 160 * side + 160)
        return part[j, half, block, :].astype(F32) + pin[j, half, block, :].astype(F32)

    def sum_index(direction, step, side, half):
        return (direction * 8 + step * 2 + side) * 2 + half

    def sum_send(direction, step, side, half, value):
        index = sum_index(direction, step, side, half)
        rsend[direction, step, side, half] = value.astype(BF16)
        push(rsend.at[direction, step, side, half], rrecv.at[direction, step, side, half],
             ssend.at[index], srecv.at[index], up if direction == 0 else down)

    def sum_take(direction, step, side, half):
        index = sum_index(direction, step, side, half)
        await_in(rrecv.at[direction, step, side, half], ssend.at[index], srecv.at[index])
        return rrecv[direction, step, side, half].astype(F32)

    def target(direction, side, step):
        j = (4 if (direction, side) in far else 3) - step
        return j % NY if direction == 0 else -j % NY

    def sum_start(half, parts):
        for direction, side in parts:
            sum_send(direction, 0, side, half,
                     chip_sum(target(direction, side, 0), half, side))

    def sum_hop(step, half, parts):
        for direction, side in parts:
            value = sum_take(direction, step - 1, side, half)
            sum_send(direction, step, side, half,
                     value + chip_sum(target(direction, side, step), half, side))

    rows_hop(1, 0)
    rows_hop(1, 1)
    expert_in(0, 0)
    expert_in(1, 0)
    rows_hop(2, 0)
    expert_in(0, 1, 7)
    rows_hop(2, 1)
    pack(1)
    for sub in range(2):
        pair_send(xs, 4, sub, psend, precv)

    for dz in range(1, NZ):
        @pl.when(z >= dz)
        def _():
            await_in(sz.at[lax.rem(z + NZ - dz, NZ)], zsend.at[dz], zrecv.at[dz])

    before, _ = prefix(sz, NZ, z)
    incoming = step(before, inside_x)[1]
    result = qd_v[0] + nt_dot(qd_v[1], incoming, HIGH)
    inverse = lax.rsqrt(jnp.mean(result * result, axis=1, keepdims=True) + EPS)
    head_out = result * inverse * hgain_ref[...] * jax.nn.silu(mixer_v[3].astype(F32))
    hs[y, c] = head_out.astype(BF16).reshape(2, ROWS // 2, DK)

    gather_start(hs, hsend, hrecv, gsend, grecv)
    expert_in(1, 1, 7)
    for copy in weights_in[2:]:
        copy.wait()

    slot0 = (e0 * RBLK + rank0).astype(F32)
    slot1 = (e1 * RBLK + rank1).astype(F32)
    which = iota((DK, ROWS), 0)
    table = jnp.where(which == 0, slot0, jnp.where(which == 1, slot1, jnp.where(
        which == 2, rw_ref[0:1, :], jnp.where(which == 3, rw_ref[1:2, :], 0.0))))
    table = jnp.transpose(table)
    place0, place1 = table[:, 0:1].astype(I32), table[:, 1:2].astype(I32)
    for g in range(N_EP * RBLK // 256):
        spot = iota((ROWS, 256), 1) + 256 * g
        weight = jnp.where(spot == place0, table[:, 2:3], 0.0) + jnp.where(
            spot == place1, table[:, 3:4], 0.0)
        high = weight.astype(BF16)
        qh_v[:, 256 * g:256 * g + 256] = high
        ql_v[:, 256 * g:256 * g + 256] = (weight - high.astype(F32)).astype(BF16)

    rows_hop(3, 0)
    expert_in(0, 2, 6, 4)
    expert_in(1, 2, 6)
    expert_in(0, 3, 5)
    expert_hidden(0)
    expert_out(0, 4)
    rows_hop(3, 1)
    expert_out(0, 3, 5)
    expert_in(1, 4)
    sum_start(0, far)
    expert_in(1, 3, 5)
    sum_start(0, near)
    expert_hidden(1)
    expert_out(1, 4, 3, 5)
    gather_hop(hs, 1, hsend, hrecv, gsend, grecv)
    expert_out(0, 2, 6)
    sum_start(1, far)
    sum_start(1, near)
    expert_out(1, 2, 6)

    def project(j):
        for sub in range(2):
            pair_take(hs, j, sub, gsend, grecv)
        heads = hs[slab(j)].reshape(2, ROWS, DK)
        rows = jnp.concatenate([heads[0], heads[1]], axis=1)
        return mm(rows, wmix_v[pl.ds(pl.multiple_of(slab(j) * FPD, FPD), FPD), :])

    row, col = iota((4 * RBLK, 4 * CAP), 0), iota((4 * RBLK, 4 * CAP), 1)
    group = (row * 2731) >> 16
    spread = ones_where((col == row - (RBLK - CAP) * group) & (row - RBLK * group < CAP))

    def give_back(o, half):
        there = 16 * half + lax.rem(me + o, 16)
        return remote(rout.at[lax.rem(there + x, 2) * 16 + lax.div(there, 2)], rin.at[me],
                      bsend.at[16 * half + o], brecv.at[me], at_ep(there))

    def finish(half):
        for side in range(2):
            value = chip_sum(0, half, side)
            for direction in range(2):
                value = value + sum_take(direction, 3 if (direction, side) in far else 2,
                                         side, half)
            for g in range(2):
                place = 16 * side + 8 * half + 4 * g
                rout[place:place + 4] = mm(
                    spread, value[80 * g:80 * g + 80].astype(BF16)
                ).astype(BF16).reshape(4, RBLK, DK)
        for o in BACK_ORDER:
            if o:
                give_back(o, half).start()
            else:
                @pl.when(lax.div(me, 16) != half)
                def _():
                    give_back(0, half).start()

    sum_hop(1, 0, far)
    expert_out(0, 1, 7, 0)
    sum_hop(1, 0, near)
    sum_hop(1, 1, far)
    expert_out(1, 1, 7, 0)
    sum_hop(1, 1, near)
    mixed = project(0)
    for half in range(2):
        sum_hop(2, half, far)
        sum_hop(2, half, near)
    mixed += project(1) + project(7)
    sum_hop(3, 0, far)
    sum_hop(3, 1, far)
    gather_hop(hs, 2, hsend, hrecv, gsend, grecv)
    finish(0)
    finish(1)
    gather_hop(hs, 3, hsend, hrecv, gsend, grecv)
    mixed += project(2) + project(6)
    gather_hop(hs, 4, hsend, hrecv, gsend, grecv)
    rin[me] = rout[lax.div(me, 2)]
    mixed += project(3) + project(5) + project(4)
    mixed_ref[...] = mixed.astype(BF16)

    for o in RETURN_ORDER:
        there = lax.rem(me + o, N_EP)
        await_in(rin.at[there], bsend.at[o], brecv.at[there])
    returned = rin[...].reshape(N_EP * RBLK, DK)
    moe_ref[...] = (mm(qh_v[...], returned) + mm(ql_v[...], returned)).astype(BF16)

    for copy in pending:
        copy.wait_send()
    for k in range(2):
        for o in SEND_ORDER:
            if o:
                dispatch(k, o).wait_send()
            else:
                @pl.when(c == 1)
                def _():
                    dispatch(k, 0).wait_send()
    for dz in range(1, NZ):
        @pl.when(z + dz < NZ)
        def _():
            along_z(dz).wait_send()

    for half in range(2):
        for o in BACK_ORDER:
            if o:
                give_back(o, half).wait_send()
            else:
                @pl.when(lax.div(me, 16) != half)
                def _():
                    give_back(0, half).wait_send()

def settle(a_ref, b_ref, mixed_ref, moe_ref):
    mixed_ref[...] = a_ref[...]
    moe_ref[...] = b_ref[...]


def body(
    mix_query, forget_input, mix_value, out_gate_input, decay_shift, forget_floor, head_gain,
    w_mix_out, moe_input, moe_gain, routes, route_weight, w_exp_gate, w_exp_up, w_exp_down,
):
    vmem = pl.BlockSpec(memory_space=pltpu.VMEM)
    hbm = pl.BlockSpec(memory_space=pl.ANY)
    sem = pltpu.SemaphoreType.DMA
    outs = jax.ShapeDtypeStruct((ROWS, DK), BF16)
    parts = pl.pallas_call(
        kernel,
        out_shape=(outs, outs),
        in_specs=[hbm] * 15,
        out_specs=(vmem, vmem),
        scratch_shapes=[
            pltpu.VMEM((1, ROWS), F32),
            pltpu.VMEM((1, DK), F32),
            pltpu.VMEM((1, DK), F32),
            pltpu.VMEM((1, D), F32),
            pltpu.VMEM((2, ROWS), I32),
            pltpu.VMEM((2, ROWS), F32),
            pltpu.VMEM((4, ROWS, DK), BF16),
            pltpu.VMEM((ROWS, D), BF16),
            pltpu.VMEM((2, ROWS, FPD), BF16),
            pltpu.VMEM((D, FPD), BF16),
            pltpu.VMEM((D, FPD), BF16),
            pltpu.VMEM((NY, FPD, FPD), BF16),
            pltpu.VMEM((D, DK), BF16),
            pltpu.VMEM((2, ROWS, FPD), BF16),
            pltpu.VMEM((2, 16, DBLK, DK), BF16),
            pltpu.VMEM((2, 16, DBLK, DK), BF16),
            pltpu.VMEM((NY, 2, 2, HALF // 2, FPD), BF16),
            pltpu.VMEM((2, HALF, FPD), F32),
            pltpu.VMEM((2, HALF, FPD), F32),
            pltpu.VMEM((2, HALF, FPD), BF16),
            pltpu.VMEM((NY, 2, HALF, DK), BF16),
            pltpu.VMEM((NY, 2, HALF, DK), BF16),
            pltpu.VMEM((NY, 2, HALF, DK), BF16),
            pltpu.VMEM((2, 4, 2, 2, HALF // 2, DK), BF16),
            pltpu.VMEM((2, 4, 2, 2, HALF // 2, DK), BF16),
            pltpu.VMEM((N_EP, RBLK, DK), BF16),
            pltpu.VMEM((N_EP, RBLK, DK), BF16),
            pltpu.VMEM((ROWS, N_EP * RBLK), BF16),
            pltpu.VMEM((ROWS, N_EP * RBLK), BF16),
            pltpu.VMEM((NX, PACK, DK), BF16),
            pltpu.VMEM((NZ, PACK, DK), BF16),
            pltpu.VMEM((2, ROWS, DK), F32),
            pltpu.VMEM((NY, 2, 2, ROWS // 2, DK), BF16),
            sem((18,)), sem((19,)), sem((32,)), sem((32,)), sem((16,)), sem((16,)),
            sem((16,)), sem((16,)), sem((16,)), sem((16,)), sem((32,)), sem((32,)),
            sem((N_EP,)), sem((N_EP,)), sem((NX,)), sem((NX,)), sem((NZ,)), sem((NZ,)),
            sem((16,)), sem((16,)), sem((16,)), sem((16,)),
        ],
        compiler_params=pltpu.CompilerParams(collective_id=0, has_side_effects=True),
        name="step",
    )(
        mix_query, forget_input, mix_value, out_gate_input,
        decay_shift.reshape(1, ROWS), forget_floor.reshape(1, DK), head_gain.reshape(1, DK),
        w_mix_out, moe_input, moe_gain.reshape(1, D), routes.T, route_weight.T,
        w_exp_gate[0], w_exp_up[0], w_exp_down[0],
    )
    return pl.pallas_call(
        settle,
        out_shape=(outs, outs),
        in_specs=[vmem] * 2,
        out_specs=(vmem, vmem),
        name="settle",
    )(*parts)


def solution(mesh):
    torus = Mesh(mesh.devices.reshape(NZ, NX, NY, 2), ("ep_0", "ep_1", "tp_0", "tp_1"))
    placed = (
        P(EP, TP), P(EP, TP), P(EP, TP), P(EP, TP), P(EP, TP), P(TP), P(), P(None, TP),
        P(EP, None), P(), P(EP, None), P(EP, None), P(EP, None, TP), P(EP, None, TP),
        P(EP, TP, None),
    )
    return jax.shard_map(
        body, mesh=torus, in_specs=placed, out_specs=(P(EP, TP), P(EP, TP)), check_vma=False
    )
```

```python
import jax
import jax.numpy as jnp
from jax import lax
from jax.experimental import pallas as pl
from jax.experimental.pallas import tpu as pltpu
from jax.sharding import Mesh
from jax.sharding import PartitionSpec as P

EP = ("ep_0", "ep_1")
TP = ("tp_0", "tp_1")
NZ, NX, NY = 8, 4, 8
N_EP = NZ * NX
ROWS = 256
CAP = 20
D = 2048
DK = 128
FPD = 256
HALF = CAP * N_EP // 2
SLOTS = CAP * N_EP
DBLK = 40
RBLK = 24
SUB = 64
PACK = DK + 16
EPS = 1e-6
MESH = pl.DeviceIdType.MESH
F32 = jnp.float32
BF16 = jnp.bfloat16
I32 = jnp.int32
HIGH = lax.Precision.HIGHEST

SEND_ORDER = (8, 7, 9, 6, 10, 5, 11, 4, 12, 3, 13, 2, 14, 1, 15, 0)
BACK_ORDER = (8, 9, 7, 10, 6, 11, 5, 12, 4, 13, 3, 14, 2, 15, 1, 0)
RETURN_ORDER = sorted(range(1, N_EP), key=lambda o: -min(o, N_EP - o))


def ones_where(mask):
    return jnp.where(mask, 1.0, 0.0).astype(BF16)


def nt_dot(a, b, precision=None):
    return lax.dot_general(
        a, b, (((1,), (1,)), ((), ())), precision=precision, preferred_element_type=F32
    )


def mm(a, b, precision=None):
    return jnp.dot(a, b, precision=precision, preferred_element_type=F32)


def iota(shape, dim):
    return lax.broadcasted_iota(I32, shape, dim)


def kernel(
    q_hbm, f_hbm, v_hbm, og_hbm, shift_hbm, floor_hbm, hgain_hbm, wmix_hbm,
    moe_hbm, gain_hbm, routes_hbm, rw_hbm, wg_hbm, wu_hbm, wd_hbm,
    mixed_ref, moe_ref,
    shift_ref, floor_ref, hgain_ref, gain_ref, routes_ref, rw_ref,
    mixer_v, moe_v, mine_v, wg_v, wu_v, wd_v, wmix_v, norm_v,
    sbuf, rbuf, xs, accg, accu, hid, part, pout, pin, rsend, rrecv,
    rout, rin, qh_v, ql_v, sx, sz, qd_v, hs,
    lsem, wsem, dsend, drecv, asend, arecv, psend, precv, csend, crecv,
    ssend, srecv, bsend, brecv, xsend, xrecv, zsend, zrecv, hsend, hrecv,
    gsend, grecv,
):
    z = lax.axis_index("ep_0")
    x = lax.axis_index("ep_1")
    y = lax.axis_index("tp_0")
    c = lax.axis_index("tp_1")
    me = z * NX + x

    def place_of(e):
        row = lax.div(e, NX)
        return lax.rem(row, 2) * 8 + lax.div(row, 2) * 2 + lax.rem(lax.div(e, 2), 2)

    def at_ep(e):
        return (lax.div(e, NX), lax.rem(e, NX), y, c)

    up = (z, x, lax.rem(y + 1, NY), c)
    down = (z, x, lax.rem(y + NY - 1, NY), c)
    partner = (z, x, y, 1 - c)

    def remote(src, dst, send, recv, device):
        return pltpu.make_async_remote_copy(
            src_ref=src, dst_ref=dst, send_sem=send, recv_sem=recv,
            device_id=device, device_id_type=MESH,
        )

    pending = []

    def push(src, dst, send, recv, device):
        copy = remote(src, dst, send, recv, device)
        copy.start()
        pending.append(copy)

    def await_in(dst, send, recv):
        remote(dst, dst, send, recv, partner).wait_recv()

    first_in = [
        pltpu.make_async_copy(routes_hbm, routes_ref, lsem.at[12]),
        pltpu.make_async_copy(gain_hbm, gain_ref, lsem.at[13])]
    for copy in first_in:
        copy.start()
    rows_in = []
    for i in range(4):
        rows_in.append(pltpu.make_async_copy(
            moe_hbm.at[pl.ds(64 * i, 64), :], moe_v.at[pl.ds(64 * i, 64), :], lsem.at[i]))
    rows_in.append(pltpu.make_async_copy(
        moe_hbm.at[:, pl.ds(pl.multiple_of(y * FPD, FPD), FPD)], mine_v.at[0], lsem.at[4]))
    rows_in.append(pltpu.make_async_copy(
        moe_hbm.at[:, pl.ds(pl.multiple_of(lax.rem(y + NY // 2, NY) * FPD, FPD), FPD)],
        mine_v.at[1], lsem.at[6]))
    for copy in rows_in:
        copy.start()
    mixer_in = [
        pltpu.make_async_copy(ref, mixer_v.at[i], lsem.at[7 + i])
        for i, ref in enumerate((f_hbm, v_hbm, q_hbm, og_hbm))]
    mixer_in += [
        pltpu.make_async_copy(a, b, lsem.at[14 + i])
        for i, (a, b) in enumerate((
            (shift_hbm, shift_ref), (floor_hbm, floor_ref), (hgain_hbm, hgain_ref),
            (rw_hbm, rw_ref)))]
    for copy in mixer_in:
        copy.start()

    barrier = pltpu.get_barrier_semaphore()

    def greet(o, carry):
        pl.semaphore_signal(
            barrier, inc=1, device_id=at_ep(lax.rem(me + o, N_EP)), device_id_type=MESH)
        return carry

    lax.fori_loop(1, N_EP, greet, 0)
    for device in (up, down, partner):
        pl.semaphore_signal(barrier, inc=1, device_id=device, device_id_type=MESH)

    weights_in = [
        pltpu.make_async_copy(wg_hbm, wg_v, wsem.at[0]),
        pltpu.make_async_copy(wu_hbm, wu_v, wsem.at[1]),
        pltpu.make_async_copy(wmix_hbm, wmix_v, wsem.at[2]),
    ]
    for i in range(NY):
        for h in range(2):
            column = pl.multiple_of(i * FPD + lax.rem(c + h, 2) * DK, DK)
            weights_in.append(pltpu.make_async_copy(
                wd_hbm.at[:, pl.ds(column, DK)],
                wd_v.at[i, :, pl.ds(h * DK, DK)], wsem.at[3 + 2 * i + h]))
    for copy in weights_in:
        copy.start()

    first_in[0].wait()
    e0, e1 = routes_ref[0:1, :], routes_ref[1:2, :]
    ids = iota((N_EP, ROWS), 0)
    one0, one1 = ids == e0, ids == e1
    ones = jnp.concatenate([ones_where(one0), ones_where(one1)], axis=0)
    strict = ones_where(iota((ROWS, ROWS), 0) < iota((ROWS, ROWS), 1))
    earlier = mm(ones, strict)
    total0 = jnp.sum(jnp.where(one0, 1.0, 0.0), axis=1, keepdims=True)
    rank0 = jnp.sum(jnp.where(one0, earlier[:N_EP], 0.0), axis=0, keepdims=True).astype(I32)
    rank1 = jnp.sum(
        jnp.where(one1, earlier[N_EP:] + total0, 0.0), axis=0, keepdims=True).astype(I32)

    parity = lax.rem(x + c, 2)
    target0 = jnp.where((e0 & 1) == parity, (e0 >> 1) * DBLK + rank0, -1000)
    target1 = jnp.where((e1 & 1) == parity, (e1 >> 1) * DBLK + rank1, -1000)
    halves = (y, lax.rem(y + NY // 2, NY))
    first_in[1].wait()
    inverses = []
    for i in range(4):
        rows_in[i].wait()
        block = moe_v[64 * i:64 * i + 64, :].astype(F32)
        mean = jnp.sum(block * block, axis=1, keepdims=True) * (1.0 / D)
        inverses.append(lax.rsqrt(mean + EPS))

    def fill(k):
        rows_in[4 + k].wait()
        gain = gain_ref[:, pl.ds(pl.multiple_of(halves[k] * FPD, FPD), FPD)]
        for i in range(4):
            own = mine_v[k, 64 * i:64 * i + 64, :].astype(F32)
            norm_v[k, 64 * i:64 * i + 64, :] = (own * inverses[i] * gain).astype(BF16)
        n0, n1 = norm_v[k, :, :DK], norm_v[k, :, DK:]
        for g in range(4):
            spot = iota((4 * DBLK, ROWS), 0) + 4 * DBLK * g
            first = ones_where((spot == target0) | (spot == target1))
            second = ones_where((spot == target0 + CAP) | (spot == target1 + CAP))
            rows = (mm(first, n0) + mm(second, n1)).astype(BF16)
            sbuf[k, 4 * g:4 * g + 4] = rows.reshape(4, DBLK, DK)

    fill(0)
    pl.semaphore_wait(barrier, N_EP + 2)

    def dispatch(k, o):
        expert = lax.rem(me + 2 * o + c, N_EP)
        return remote(sbuf.at[k, lax.div(expert, 2)], rbuf.at[k, place_of(me)],
                      dsend.at[16 * k + o], drecv.at[16 * k + o], at_ep(expert))

    own_copies = [pltpu.make_async_copy(
        sbuf.at[k, lax.div(me, 2)], rbuf.at[k, place_of(me)], lsem.at[k * 6 + 5])
        for k in range(2)]
    for k in range(2):
        if k:
            fill(k)
        for o in SEND_ORDER:
            if o:
                dispatch(k, o).start()
            else:
                @pl.when(c == 1)
                def _():
                    dispatch(k, 0).start()

                @pl.when(c == 0)
                def _():
                    own_copies[k].start()

    for copy in mixer_in:
        copy.wait()
    floor = floor_ref[...]
    pre = mixer_v[0].astype(F32)
    forget = floor + (1.0 - floor) * jax.nn.sigmoid(pre)
    keys = (1.0 - floor) * jax.nn.sigmoid(-pre)
    shift = jnp.transpose(jnp.broadcast_to(shift_ref[...], (DK, ROWS)))
    log_decay = jnp.log(forget) + shift
    lower = jnp.where(iota((ROWS, ROWS), 0) >= iota((ROWS, ROWS), 1), 1.0, 0.0)
    running = mm(lower, log_decay, HIGH)
    values = mixer_v[1].astype(F32)
    query = mixer_v[2].astype(F32)
    closing = running[ROWS - 1:ROWS, :]
    values_t = jnp.transpose(values)
    state_t = mm(values_t, keys * jnp.exp(closing - running), HIGH)
    sx[x, 0:DK, :] = state_t.astype(BF16)
    sx[x, DK:PACK, :] = jnp.broadcast_to(jnp.exp(closing), (PACK - DK, DK)).astype(BF16)
    for dx in range(1, NX):
        push(sx.at[x], sx.at[x], xsend.at[dx], xrecv.at[dx],
             (z, lax.rem(x + dx, NX), y, c))

    def arrived(k):
        for o in SEND_ORDER:
            source = lax.rem(me + N_EP - 2 * o + N_EP - c, N_EP)
            slot = rbuf.at[k, place_of(source)]
            if o:
                await_in(slot, dsend.at[16 * k + o], drecv.at[16 * k + o])
            else:
                @pl.when(c == 1)
                def _():
                    await_in(slot, dsend.at[16 * k], drecv.at[16 * k])

                @pl.when(c == 0)
                def _():
                    own_copies[k].wait()

    row, col = iota((4 * CAP, 4 * DBLK), 0), iota((4 * CAP, 4 * DBLK), 1)
    spot = row + (DBLK - CAP) * ((row * 3277) >> 16)
    packs = [ones_where(col == spot + CAP * h) for h in range(2)]

    def pack(k):
        arrived(k)
        for g in range(4):
            block = rbuf[k, 4 * g:4 * g + 4].reshape(4 * DBLK, DK)
            for h in range(2):
                xs[halves[k], c, g // 2, (g % 2) * 80:(g % 2) * 80 + 80,
                   h * DK:(h + 1) * DK] = mm(packs[h], block).astype(BF16)

    pack(0)

    def slab(j):
        return lax.rem(y + j, NY)

    def ring_send(buf, direction, hop, sub, send, recv):
        j = (NY - hop) % NY if direction == 0 else hop
        index = direction * 8 + hop * 2 + sub
        push(buf.at[slab(j), c, sub], buf.at[slab(j), c, sub], send.at[index], recv.at[index],
             up if direction == 0 else down)

    def ring_take(buf, direction, hop, sub, send, recv):
        j = (NY - hop) % NY if direction == 0 else hop
        index = direction * 8 + (hop - 1) * 2 + sub
        await_in(buf.at[slab(j), c, sub], send.at[index], recv.at[index])
        return j

    def pair_send(buf, j, sub, send, recv):
        push(buf.at[slab(j), c, sub], buf.at[slab(j), c, sub],
             send.at[2 * j + sub], recv.at[2 * j + sub], partner)

    def pair_take(buf, j, sub, send, recv):
        await_in(buf.at[slab(j), 1 - c, sub], send.at[2 * j + sub], recv.at[2 * j + sub])

    far, near = ((0, 0), (1, 1)), ((0, 1), (1, 0))

    def gather_start(buf, send, recv, psend, precv):
        for direction, sub in far + near:
            ring_send(buf, direction, 0, sub, send, recv)
        for sub in range(2):
            pair_send(buf, 0, sub, psend, precv)

    def gather_hop(buf, hop, send, recv, psend, precv):
        for direction, sub in far + (near if hop < 4 else ()):
            j = ring_take(buf, direction, hop, sub, send, recv)
            if hop < (4 if (direction, sub) in far else 3):
                ring_send(buf, direction, hop, sub, send, recv)
            pair_send(buf, j, sub, psend, precv)

    for sub in range(2):
        for direction in range(2):
            ring_send(xs, direction, 0, sub, asend, arecv)
        pair_send(xs, 0, sub, psend, precv)

    def rows_hop(hop, sub):
        for direction in range(2):
            j = ring_take(xs, direction, hop, sub, asend, arecv)
            if hop < 3:
                ring_send(xs, direction, hop, sub, asend, arecv)
            pair_send(xs, j, sub, psend, precv)


    def read_state(ref, k):
        return ref[k, DK:PACK, :].astype(F32)[0:1], ref[k, 0:DK, :].astype(F32)

    def step(before, after):
        return before[0] * after[0], after[0] * before[1] + after[1]

    def prefix(ref, count, index):
        running = (jnp.ones((1, DK), F32), jnp.zeros((DK, DK), F32))
        inside = running
        for k in range(count):
            running = step(running, read_state(ref, k))
            inside = tuple(jnp.where(k < index, a, b) for a, b in zip(running, inside))
        return inside, running

    for dx in range(1, NX):
        await_in(sx.at[lax.rem(x + NX - dx, NX)], xsend.at[dx], xrecv.at[dx])
    inside_x, whole = prefix(sx, NX, x)
    sz[z, 0:DK, :] = whole[1].astype(BF16)
    sz[z, DK:PACK, :] = jnp.broadcast_to(whole[0], (PACK - DK, DK)).astype(BF16)

    def along_z(dz):
        return remote(sz.at[z], sz.at[z], zsend.at[dz], zrecv.at[dz],
                      (lax.rem(z + dz, NZ), x, y, c))

    for dz in range(1, NZ):
        @pl.when(z + dz < NZ)
        def _():
            along_z(dz).start()

    causal = iota((SUB, SUB), 0) >= iota((SUB, SUB), 1)
    local = []
    for i in range(ROWS // SUB):
        lo, hi = i * SUB, (i + 1) * SUB
        decay_i, query_i = running[lo:hi], query[lo:hi]
        middle = running[lo + SUB // 2 - 1:lo + SUB // 2]
        scores = jnp.where(causal, nt_dot(
            query_i * jnp.exp(decay_i - middle), keys[lo:hi] * jnp.exp(middle - decay_i),
            HIGH), 0.0)
        out = mm(scores, values[lo:hi], HIGH)
        if i:
            start = running[lo - 1:lo]
            scores = nt_dot(query_i * jnp.exp(decay_i - start),
                            keys[:lo] * jnp.exp(start - running[:lo]), HIGH)
            out = out + mm(scores, values[:lo], HIGH)
        local.append(out)
    qd_v[0] = jnp.concatenate(local, axis=0)
    qd_v[1] = query * jnp.exp(running)


    weights_in[0].wait()
    weights_in[1].wait()

    def expert_in(half, *slabs):
        for j in slabs:
            pair_take(xs, j, half, psend, precv)
            rows = jnp.concatenate([xs[slab(j), 0, half], xs[slab(j), 1, half]], axis=0)
            depth = pl.ds(pl.multiple_of(slab(j) * FPD, FPD), FPD)
            gate, raised = mm(rows, wg_v[depth, :]), mm(rows, wu_v[depth, :])
            if j == 0:
                accg[half], accu[half] = gate, raised
            else:
                accg[half] += gate
                accu[half] += raised

    def expert_hidden(half):
        for i in range(2):
            block = slice(160 * i, 160 * i + 160)
            hid[half, block, :] = (
                jax.nn.silu(accg[half, block, :]) * accu[half, block, :]).astype(BF16)

    def expert_out(half, *slabs):
        for j in slabs:
            partial = mm(hid[half], wd_v[slab(j)]).astype(BF16)
            part[j, half] = partial[:, :DK]
            pout[j, half] = partial[:, DK:]
            push(pout.at[j, half], pin.at[j, half],
                 csend.at[2 * j + half], crecv.at[2 * j + half], partner)

    summed = set()

    def chip_sum(j, half, side):
        if (j, half) not in summed:
            summed.add((j, half))
            await_in(pin.at[j, half], csend.at[2 * j + half], crecv.at[2 * j + half])
        block = slice(160 * side, 160 * side + 160)
        return part[j, half, block, :].astype(F32) + pin[j, half, block, :].astype(F32)

    def sum_index(direction, step, side, half):
        return (direction * 8 + step * 2 + side) * 2 + half

    def sum_send(direction, step, side, half, value):
        index = sum_index(direction, step, side, half)
        rsend[direction, step, side, half] = value.astype(BF16)
        push(rsend.at[direction, step, side, half], rrecv.at[direction, step, side, half],
             ssend.at[index], srecv.at[index], up if direction == 0 else down)

    def sum_take(direction, step, side, half):
        index = sum_index(direction, step, side, half)
        await_in(rrecv.at[direction, step, side, half], ssend.at[index], srecv.at[index])
        return rrecv[direction, step, side, half].astype(F32)

    def target(direction, side, step):
        j = (4 if (direction, side) in far else 3) - step
        return j % NY if direction == 0 else -j % NY

    def sum_start(half, parts):
        for direction, side in parts:
            sum_send(direction, 0, side, half,
                     chip_sum(target(direction, side, 0), half, side))

    def sum_hop(step, half, parts):
        for direction, side in parts:
            value = sum_take(direction, step - 1, side, half)
            sum_send(direction, step, side, half,
                     value + chip_sum(target(direction, side, step), half, side))

    rows_hop(1, 0)
    rows_hop(1, 1)
    expert_in(0, 0)
    expert_in(1, 0)
    rows_hop(2, 0)
    expert_in(0, 1, 7)
    rows_hop(2, 1)
    pack(1)
    for sub in range(2):
        pair_send(xs, 4, sub, psend, precv)

    for dz in range(1, NZ):
        @pl.when(z >= dz)
        def _():
            await_in(sz.at[lax.rem(z + NZ - dz, NZ)], zsend.at[dz], zrecv.at[dz])

    before, _ = prefix(sz, NZ, z)
    incoming = step(before, inside_x)[1]
    result = qd_v[0] + nt_dot(qd_v[1], incoming, HIGH)
    inverse = lax.rsqrt(jnp.mean(result * result, axis=1, keepdims=True) + EPS)
    head_out = result * inverse * hgain_ref[...] * jax.nn.silu(mixer_v[3].astype(F32))
    hs[y, c] = head_out.astype(BF16).reshape(2, ROWS // 2, DK)

    gather_start(hs, hsend, hrecv, gsend, grecv)
    expert_in(1, 1, 7)
    for copy in weights_in[2:]:
        copy.wait()

    slot0 = (e0 * RBLK + rank0).astype(F32)
    slot1 = (e1 * RBLK + rank1).astype(F32)
    which = iota((DK, ROWS), 0)
    table = jnp.where(which == 0, slot0, jnp.where(which == 1, slot1, jnp.where(
        which == 2, rw_ref[0:1, :], jnp.where(which == 3, rw_ref[1:2, :], 0.0))))
    table = jnp.transpose(table)
    place0, place1 = table[:, 0:1].astype(I32), table[:, 1:2].astype(I32)
    for g in range(N_EP * RBLK // 256):
        spot = iota((ROWS, 256), 1) + 256 * g
        weight = jnp.where(spot == place0, table[:, 2:3], 0.0) + jnp.where(
            spot == place1, table[:, 3:4], 0.0)
        high = weight.astype(BF16)
        qh_v[:, 256 * g:256 * g + 256] = high
        ql_v[:, 256 * g:256 * g + 256] = (weight - high.astype(F32)).astype(BF16)

    rows_hop(3, 0)
    expert_in(0, 2, 6, 4)
    expert_in(1, 2, 6)
    expert_in(0, 3, 5)
    expert_hidden(0)
    expert_out(0, 4)
    rows_hop(3, 1)
    expert_out(0, 3, 5)
    expert_in(1, 4)
    sum_start(0, far)
    expert_in(1, 3, 5)
    sum_start(0, near)
    expert_hidden(1)
    expert_out(1, 4, 3, 5)
    gather_hop(hs, 1, hsend, hrecv, gsend, grecv)
    expert_out(0, 2, 6)
    sum_start(1, far)
    sum_start(1, near)
    expert_out(1, 2, 6)

    def project(j):
        for sub in range(2):
            pair_take(hs, j, sub, gsend, grecv)
        heads = hs[slab(j)].reshape(2, ROWS, DK)
        rows = jnp.concatenate([heads[0], heads[1]], axis=1)
        return mm(rows, wmix_v[pl.ds(pl.multiple_of(slab(j) * FPD, FPD), FPD), :])

    row, col = iota((4 * RBLK, 4 * CAP), 0), iota((4 * RBLK, 4 * CAP), 1)
    group = (row * 2731) >> 16
    spread = ones_where((col == row - (RBLK - CAP) * group) & (row - RBLK * group < CAP))

    def give_back(o, half):
        spot = lax.rem(lax.div(z, 2) * NX + x + o, 16)
        there = (lax.div(spot, NX) * 2 + half) * NX + lax.rem(spot, NX)
        return remote(rout.at[lax.rem(there + x, 2) * 16 + place_of(there)], rin.at[me],
                      bsend.at[16 * half + o], brecv.at[me], at_ep(there))

    def finish(half):
        for side in range(2):
            value = chip_sum(0, half, side)
            for direction in range(2):
                value = value + sum_take(direction, 3 if (direction, side) in far else 2,
                                         side, half)
            for g in range(2):
                place = 16 * side + 8 * half + 4 * g
                rout[place:place + 4] = mm(
                    spread, value[80 * g:80 * g + 80].astype(BF16)
                ).astype(BF16).reshape(4, RBLK, DK)
        for o in BACK_ORDER:
            if o:
                give_back(o, half).start()
            else:
                @pl.when(lax.rem(z, 2) != half)
                def _():
                    give_back(0, half).start()

    sum_hop(1, 0, far)
    expert_out(0, 1, 7, 0)
    sum_hop(1, 0, near)
    sum_hop(1, 1, far)
    expert_out(1, 1, 7, 0)
    sum_hop(1, 1, near)
    mixed = project(0)
    for half in range(2):
        sum_hop(2, half, far)
        sum_hop(2, half, near)
    mixed += project(1) + project(7)
    sum_hop(3, 0, far)
    sum_hop(3, 1, far)
    gather_hop(hs, 2, hsend, hrecv, gsend, grecv)
    finish(0)
    finish(1)
    gather_hop(hs, 3, hsend, hrecv, gsend, grecv)
    mixed += project(2) + project(6)
    gather_hop(hs, 4, hsend, hrecv, gsend, grecv)
    rin[me] = rout[place_of(me)]
    mixed += project(3) + project(5) + project(4)
    mixed_ref[...] = mixed.astype(BF16)

    for o in RETURN_ORDER:
        there = lax.rem(me + o, N_EP)
        await_in(rin.at[there], bsend.at[o], brecv.at[there])
    returned = rin[...].reshape(N_EP * RBLK, DK)
    moe_ref[...] = (mm(qh_v[...], returned) + mm(ql_v[...], returned)).astype(BF16)

    for copy in pending:
        copy.wait_send()
    for k in range(2):
        for o in SEND_ORDER:
            if o:
                dispatch(k, o).wait_send()
            else:
                @pl.when(c == 1)
                def _():
                    dispatch(k, 0).wait_send()
    for dz in range(1, NZ):
        @pl.when(z + dz < NZ)
        def _():
            along_z(dz).wait_send()

    for half in range(2):
        for o in BACK_ORDER:
            if o:
                give_back(o, half).wait_send()
            else:
                @pl.when(lax.rem(z, 2) != half)
                def _():
                    give_back(0, half).wait_send()

def settle(a_ref, b_ref, mixed_ref, moe_ref):
    mixed_ref[...] = a_ref[...]
    moe_ref[...] = b_ref[...]


def body(
    mix_query, forget_input, mix_value, out_gate_input, decay_shift, forget_floor, head_gain,
    w_mix_out, moe_input, moe_gain, routes, route_weight, w_exp_gate, w_exp_up, w_exp_down,
):
    vmem = pl.BlockSpec(memory_space=pltpu.VMEM)
    hbm = pl.BlockSpec(memory_space=pl.ANY)
    sem = pltpu.SemaphoreType.DMA
    outs = jax.ShapeDtypeStruct((ROWS, DK), BF16)
    parts = pl.pallas_call(
        kernel,
        out_shape=(outs, outs),
        in_specs=[hbm] * 15,
        out_specs=(vmem, vmem),
        scratch_shapes=[
            pltpu.VMEM((1, ROWS), F32),
            pltpu.VMEM((1, DK), F32),
            pltpu.VMEM((1, DK), F32),
            pltpu.VMEM((1, D), F32),
            pltpu.VMEM((2, ROWS), I32),
            pltpu.VMEM((2, ROWS), F32),
            pltpu.VMEM((4, ROWS, DK), BF16),
            pltpu.VMEM((ROWS, D), BF16),
            pltpu.VMEM((2, ROWS, FPD), BF16),
            pltpu.VMEM((D, FPD), BF16),
            pltpu.VMEM((D, FPD), BF16),
            pltpu.VMEM((NY, FPD, FPD), BF16),
            pltpu.VMEM((D, DK), BF16),
            pltpu.VMEM((2, ROWS, FPD), BF16),
            pltpu.VMEM((2, 16, DBLK, DK), BF16),
            pltpu.VMEM((2, 16, DBLK, DK), BF16),
            pltpu.VMEM((NY, 2, 2, HALF // 2, FPD), BF16),
            pltpu.VMEM((2, HALF, FPD), F32),
            pltpu.VMEM((2, HALF, FPD), F32),
            pltpu.VMEM((2, HALF, FPD), BF16),
            pltpu.VMEM((NY, 2, HALF, DK), BF16),
            pltpu.VMEM((NY, 2, HALF, DK), BF16),
            pltpu.VMEM((NY, 2, HALF, DK), BF16),
            pltpu.VMEM((2, 4, 2, 2, HALF // 2, DK), BF16),
            pltpu.VMEM((2, 4, 2, 2, HALF // 2, DK), BF16),
            pltpu.VMEM((N_EP, RBLK, DK), BF16),
            pltpu.VMEM((N_EP, RBLK, DK), BF16),
            pltpu.VMEM((ROWS, N_EP * RBLK), BF16),
            pltpu.VMEM((ROWS, N_EP * RBLK), BF16),
            pltpu.VMEM((NX, PACK, DK), BF16),
            pltpu.VMEM((NZ, PACK, DK), BF16),
            pltpu.VMEM((2, ROWS, DK), F32),
            pltpu.VMEM((NY, 2, 2, ROWS // 2, DK), BF16),
            sem((18,)), sem((19,)), sem((32,)), sem((32,)), sem((16,)), sem((16,)),
            sem((16,)), sem((16,)), sem((16,)), sem((16,)), sem((32,)), sem((32,)),
            sem((N_EP,)), sem((N_EP,)), sem((NX,)), sem((NX,)), sem((NZ,)), sem((NZ,)),
            sem((16,)), sem((16,)), sem((16,)), sem((16,)),
        ],
        compiler_params=pltpu.CompilerParams(collective_id=0, has_side_effects=True),
        name="step",
    )(
        mix_query, forget_input, mix_value, out_gate_input,
        decay_shift.reshape(1, ROWS), forget_floor.reshape(1, DK), head_gain.reshape(1, DK),
        w_mix_out, moe_input, moe_gain.reshape(1, D), routes.T, route_weight.T,
        w_exp_gate[0], w_exp_up[0], w_exp_down[0],
    )
    return pl.pallas_call(
        settle,
        out_shape=(outs, outs),
        in_specs=[vmem] * 2,
        out_specs=(vmem, vmem),
        name="settle",
    )(*parts)


def solution(mesh):
    torus = Mesh(mesh.devices.reshape(NZ, NX, NY, 2), ("ep_0", "ep_1", "tp_0", "tp_1"))
    placed = (
        P(EP, TP), P(EP, TP), P(EP, TP), P(EP, TP), P(EP, TP), P(TP), P(), P(None, TP),
        P(EP, None), P(), P(EP, None), P(EP, None), P(EP, None, TP), P(EP, None, TP),
        P(EP, TP, None),
    )
    return jax.shard_map(
        body, mesh=torus, in_specs=placed, out_specs=(P(EP, TP), P(EP, TP)), check_vma=False
    )
```
